256 devices in a mesh: sp: 64 (over z, x, core), tp: 4 (over y).
Axes of the slice: x: 4, y: 4, z: 8, core: 2. Of those that a mesh axis runs over, the one named last changes fastest.
Arguments:
- tokens: bfloat16 [16384, 1024], P(('sp', 'tp')), may hold values from -6 to 6
- norm_gain: float32 [1024], replicated, may hold values from 0.1 to 1.9
- w_query: bfloat16 [1024, 1024], P('sp', 'tp'), may hold values from -0.1875 to 0.1875
- w_key: bfloat16 [1024, 1024], P('sp', 'tp'), may hold values from -0.1875 to 0.1875
- w_value: bfloat16 [1024, 1024], P('sp', 'tp'), may hold values from -0.1875 to 0.1875
- w_forget: bfloat16 [1024, 16], P('sp', 'tp'), may hold values from -0.375 to 0.375
- forget_offset: float32 [16], P('tp'), may hold values from 1 to 3.5
- w_out_t: bfloat16 [1024, 1024], P('sp', 'tp'), may hold values from -0.1875 to 0.1875
- out_gain: float32 [1024], replicated, may hold values from 0.1 to 1.9
Outputs:
- mixed: bfloat16 [16384, 1024], P(('sp', 'tp'))
The draws below stay inside these ranges and needn't reach their ends.
All inputs are finite; a program needn't handle non-finite values.
Results may differ from the reference program's by a relative error of at most 0.015.
Values may be sent and summed in bfloat16 or wider, within the bound.
A program may use at most 192 MiB of HBM per device.

```python
import jax
import jax.numpy as jnp
from jax import lax

D = 1024
HEADS = 16
HEAD_DIM = 64
TOK_DEV = 256
TOKENS = 16384
N_SP = 64


def block_scale(key, dims, split, smallest, top_value):
    def one(axis_at, blocks):
        draws = jax.random.uniform(jax.random.fold_in(jax.random.fold_in(key, 6), axis_at), (blocks,), jnp.float32, smallest / len(split), top_value / len(split))
        return jnp.repeat(jnp.exp(draws), dims[axis_at] // blocks).reshape((-1,) + (1,) * (len(dims) - axis_at - 1))

    loudness = one(*split[0])
    for cut in split[1:]:
        loudness = loudness * one(*cut)
    return loudness


def gaussian(rng, shape, spread, limit, shards=(), kind=jnp.bfloat16):
    drawn = jax.random.normal(rng, shape, jnp.float32) * spread
    if len(shards) > 0:
        drawn = block_scale(rng, shape, shards, -0.22, 0.18) * drawn
    return jnp.clip(drawn, min=-limit, max=limit).astype(kind)


def setup_inputs(seed: int = 0) -> dict:
    streams_of = jax.random.split(jax.random.key(seed), 10)
    tokens = gaussian(streams_of[0], (TOKENS, D), 1.0, 6.0, ((0, 256),))
    norm_gain = jnp.clip(1.0 + 0.18 * jax.random.normal(streams_of[1], (D,), jnp.float32), 0.1, 1.9)
    w_query = gaussian(streams_of[2], (D, HEADS * HEAD_DIM), D ** -0.5, 0.1875, ((0, 64), (1, 4)))
    w_key = gaussian(streams_of[3], (D, HEADS * HEAD_DIM), D ** -0.5, 0.1875, ((0, 64), (1, 4)))
    w_value = gaussian(streams_of[4], (D, HEADS * HEAD_DIM), D ** -0.5, 0.1875, ((0, 64), (1, 4)))
    w_forget = gaussian(streams_of[5], (D, HEADS), (D // 4) ** -0.5, 0.375, ((0, 64), (1, 4)))
    forget_offset = jnp.clip(1.0 + 2.5 * jax.random.uniform(streams_of[6], (HEADS,), jnp.float32) ** block_scale(streams_of[6], (HEADS,), ((0, 4),), -0.2, 0.2), 1.0, 3.5)
    w_out_t = gaussian(streams_of[7], (D, HEADS * HEAD_DIM), (HEADS * HEAD_DIM) ** -0.5, 0.1875, ((0, 64), (1, 4)))
    out_gain = jnp.clip(1.0 + 0.18 * jax.random.normal(streams_of[8], (D,), jnp.float32), 0.1, 1.9)
    return {"tokens": tokens, "norm_gain": norm_gain, "w_query": w_query, "w_key": w_key, "w_value": w_value, "w_forget": w_forget, "forget_offset": forget_offset, "w_out_t": w_out_t, "out_gain": out_gain}


norm_eps = 1e-06

def rms_norm(values_in, gain_row):
    floats = values_in.astype(jnp.float32)
    scale_row = lax.rsqrt(lax.optimization_barrier(jnp.mean(floats * floats, axis=-1, keepdims=True)) + norm_eps)
    return (floats * scale_row * gain_row).astype(jnp.bfloat16)

def reference(tokens, norm_gain, w_query, w_key, w_value, w_forget, forget_offset, w_out_t, out_gain):
    normed = rms_norm(tokens, norm_gain)
    queries = jnp.dot(normed, w_query, preferred_element_type=jnp.float32).astype(jnp.bfloat16)
    keys_all = jnp.dot(normed, w_key, preferred_element_type=jnp.float32).astype(jnp.bfloat16)
    values_all = jnp.dot(normed, w_value, preferred_element_type=jnp.float32).astype(jnp.bfloat16)
    logits = jnp.dot(normed, w_forget, preferred_element_type=jnp.float32) + forget_offset + jnp.log(jnp.float32(TOKENS))
    log_gates = jax.nn.log_sigmoid(logits)
    cumulative = jnp.cumsum(log_gates, axis=0)
    head_shape = (TOKENS, HEADS, HEAD_DIM)
    key_heads = keys_all.reshape(head_shape).astype(jnp.float32)
    value_heads = values_all.reshape(head_shape).astype(jnp.float32)
    query_blocks = queries.reshape(N_SP, TOK_DEV, HEADS, HEAD_DIM).astype(jnp.float32)
    cum_blocks = cumulative.reshape(N_SP, TOK_DEV, HEADS)
    key_pos = jnp.arange(TOKENS, dtype=jnp.int32)

    def attend(block_args):
        query_block, cum_block, block_index = block_args
        scores = jnp.einsum('qhd,khd->hqk', query_block, key_heads, precision=lax.Precision.HIGHEST) * HEAD_DIM ** (-0.5)
        scores = scores + cum_block.T[:, :, None] - cumulative.T[:, None, :]
        query_pos = block_index * TOK_DEV + jnp.arange(TOK_DEV, dtype=jnp.int32)
        allowed = key_pos[None, :] <= query_pos[:, None]
        scores = jnp.where(allowed[None], scores, -jnp.inf)
        attn_probs = jax.nn.softmax(scores, axis=-1)
        return jnp.einsum('hqk,khd->qhd', attn_probs, value_heads, precision=lax.Precision.HIGHEST)
    attended = lax.map(attend, (query_blocks, cum_blocks, jnp.arange(N_SP, dtype=jnp.int32)))
    attended = attended.reshape(TOKENS, HEADS * HEAD_DIM).astype(jnp.bfloat16)
    projected = lax.dot_general(attended, w_out_t, (((1,), (1,)), ((), ())), preferred_element_type=jnp.float32)
    return rms_norm(projected, out_gain)
```

```python
import functools
import math

import jax
import jax.numpy as jnp
from jax import lax
from jax.experimental import pallas as pl
from jax.experimental.pallas import tpu as pltpu
from jax.sharding import Mesh
from jax.sharding import PartitionSpec as P

HEAD_DIM = 64
AXES = ("z", "x", "c", "y")
MESH = pl.DeviceIdType.MESH
EPS = 1e-06
LOG2E = 1.4426950408889634
LOW = -1e30
LANES = 128


def rms_norm(floats, gain_row):
    scale_row = lax.rsqrt(jnp.mean(floats * floats, axis=-1, keepdims=True) + EPS)
    return (floats * scale_row * gain_row).astype(jnp.bfloat16)


def log_sigmoid(t):
    u = jnp.exp(-jnp.abs(t))
    series = u * (1.0 - u * (0.5 - u * (1.0 / 3.0 - u * 0.25)))
    return jnp.minimum(t, 0.0) - jnp.where(u < 0.01, series, jnp.log(1.0 + u))


class Links:
    def __init__(self, send_sems, recv_sems, ids):
        self.send_sems, self.recv_sems, self.ids, self.sent = send_sems, recv_sems, ids, []

    def copy(self, key, src, dst, dev):
        at = self.ids.setdefault(key, len(self.ids))
        return pltpu.make_async_remote_copy(
            src_ref=src,
            dst_ref=dst,
            send_sem=self.send_sems.at[at],
            recv_sem=self.recv_sems.at[at],
            device_id=dev,
            device_id_type=MESH,
        )

    def send(self, key, src, dst, dev):
        c = self.copy(key, src, dst, dev)
        c.start()
        self.sent.append(c)

    def recv(self, key, landed, dev):
        self.copy(key, landed, landed, dev).wait_recv()

    def drain(self):
        for c in self.sent:
            c.wait_send()


def kernel(
    dims,
    tokens_ref,
    gain_ref,
    wcat_ref,
    off_ref,
    wo_ref,
    ogain_ref,
    out_ref,
    W,
    XN,
    WO,
    KS,
    VS,
    QS,
    GS,
    GX,
    GP,
    GPR,
    G,
    CUM,
    K,
    VT,
    QT,
    QB,
    M,
    ACC,
    OS,
    AT,
    PT,
    send_sems,
    recv_sems,
):
    Z, X, C, Y = dims
    TB, D = tokens_ref.shape
    GB = TB * Y
    HB = GB // 2
    PR, LW = wcat_ref.shape
    LH = LW // 2
    WC = wo_ref.shape[1]
    z, x, c, y = (lax.axis_index(a) for a in AXES)
    links = Links(send_sems, recv_sems, {})
    UP = Z // 2
    DN = Z - 1 - UP

    def dev(dz=0, dx=0, dc=0, dy=0):
        return {
            "z": lax.rem(z + (dz % Z), Z),
            "x": lax.rem(x + (dx % X), X),
            "c": lax.rem(c + (dc % C), C),
            "y": lax.rem(y + (dy % Y), Y),
        }

    def zrel(d):
        return lax.rem(z + (d % Z), Z)

    def xrel(d):
        return lax.rem(x + (d % X), X)

    def yrel(d):
        return lax.rem(y + (d % Y), Y)

    co = 1 - c
    plane = [(dx, dy) for dx in range(X) for dy in range(Y) if (dx, dy) != (0, 0)]

    barrier = pltpu.get_barrier_semaphore()
    greeted = (
        [dict(dx=dx, dy=dy) for dx, dy in plane]
        + [dict(dx=dx, dc=1) for dx in range(X)]
        + [dict(dz=d) for d in range(1, Z)]
    )
    for g in greeted:
        pl.semaphore_signal(barrier, inc=1, device_id=dev(**g), device_id_type=MESH)
    pl.semaphore_wait(barrier, len(greeted))

    def w_rows(zz, xx, cc):
        return pl.ds(pl.multiple_of(((zz * X + xx) * C + cc) * PR, PR), PR)

    def half(cc):
        return pl.ds(pl.multiple_of(cc * LH, LANES), LH)

    for dx in range(X):
        for dc in range(C):
            if (dx, dc) != (0, 0):
                to = half(c if dc == 0 else co)
                links.send(
                    ("wx", dx, dc), wcat_ref.at[:, to], W.at[w_rows(z, x, c), to], dev(dx=dx, dc=dc)
                )
    W[w_rows(z, x, c), half(c)] = wcat_ref[:, half(c)]

    XN[pl.ds(pl.multiple_of(y * TB, TB), TB), :] = rms_norm(
        tokens_ref[...].astype(jnp.float32), gain_ref[...]
    )
    mine = XN.at[pl.ds(pl.multiple_of(y * TB, TB), TB), :]
    for dy in range(1, Y):
        links.send(("tok", dy), mine, mine, dev(dy=dy))

    def wo_block(cc, xx, zz, yy):
        row = ((cc * X + xx) * Z + zz) * PR
        return WO.at[
            pl.ds(pl.multiple_of(row, PR), PR), pl.ds(pl.multiple_of(yy * WC, LANES), WC)
        ]

    def wo_bundle(cc, xx, yy):
        row = (cc * X + xx) * Z * PR
        return WO.at[
            pl.ds(pl.multiple_of(row, PR), Z * PR), pl.ds(pl.multiple_of(yy * WC, LANES), WC)
        ]

    wo_block(c, x, z, y)[...] = wo_ref[...]

    def ring_start(name, views):
        for a, view in enumerate(views(z, c)):
            if UP > 0:
                links.send((name, "up", 1, a), view, view, dev(dz=1))
            if DN > 0:
                links.send((name, "dn", 1, a), view, view, dev(dz=-1))
        for a, view in enumerate(views(z, c)):
            links.send((name, "core", 0, a), view, view, dev(dc=1))

    def ring_step(name, views, k):
        for a in range(len(views(z, c))):
            for way, sign, last in (("up", 1, UP), ("dn", -1, DN)):
                if k <= last:
                    view = views(zrel(-sign * k), c)[a]
                    links.recv((name, way, k, a), view, dev(dz=-sign))
                    if k < last:
                        links.send((name, way, k + 1, a), view, view, dev(dz=sign))
                    links.send((name, "core", -sign * k, a), view, view, dev(dc=1))

    def other_core(name, views, d):
        for a, view in enumerate(views(zrel(d), co)):
            links.recv((name, "core", d, a), view, dev(dc=1))

    PARTS = 2 if LH % (2 * LANES) == 0 else 1

    def w_views(zz, cc):
        rows = pl.ds(pl.multiple_of(zz * X * C * PR, X * C * PR), X * C * PR)
        step = LH // PARTS
        return [
            W.at[rows, pl.ds(pl.multiple_of(cc * LH + p * step, LANES), step)] for p in range(PARTS)
        ]

    for dx in range(X):
        for dc in range(C):
            if (dx, dc) != (0, 0):
                sx, sc = xrel(-dx), (c if dc == 0 else co)
                links.recv(("wx", dx, dc), W.at[w_rows(z, sx, sc), half(c)], dev(dx=-dx, dc=dc))
    ring_start("w", w_views)
    for d in range(1, Z):
        links.send(("woz", d), wo_ref, wo_block(c, x, z, y), dev(dz=d))
    for k in range(1, UP + 1):
        ring_step("w", w_views, k)
    for d in [0] + list(range(1, DN + 1)) + [-k for k in range(1, UP + 1)]:
        other_core("w", w_views, d)
    for dy in range(1, Y):
        landed = XN.at[pl.ds(pl.multiple_of(yrel(-dy) * TB, TB), TB), :]
        links.recv(("tok", dy), landed, dev(dy=-dy))

    rows = XN[...]
    k_all = jnp.dot(rows, W[:, WC : 2 * WC], preferred_element_type=jnp.float32)
    for h in range(X):
        kh = k_all[:, h * HEAD_DIM : (h + 1) * HEAD_DIM]
        KS[h] = jnp.concatenate([kh[:HB], kh[HB:]], axis=1).astype(jnp.bfloat16)
    v_all = jnp.dot(rows, W[:, 2 * WC : 3 * WC], preferred_element_type=jnp.float32).T
    for h in range(X):
        vh = v_all[h * HEAD_DIM : (h + 1) * HEAD_DIM].astype(jnp.bfloat16)
        VS[h, 0] = vh[:, :HB]
        VS[h, 1] = vh[:, HB:]
    gates = jnp.dot(rows, W[:, 3 * WC : 3 * WC + LANES], preferred_element_type=jnp.float32)
    gates = gates.T[:8]
    head_row = lax.broadcasted_iota(jnp.int32, gates.shape, 0)
    offset = jnp.zeros_like(gates)
    for h in range(X):
        offset = jnp.where(head_row == h, off_ref[h], offset)
    GS[...] = log_sigmoid(gates + offset + math.log(GB * Z * X * C))

    def slot(cc, zz, xx):
        return ((cc * Z + zz) * X + xx) * HB

    def k_block(cc, zz, xx):
        return K.at[pl.ds(pl.multiple_of(slot(cc, zz, xx), LANES), HB), :]

    def v_block(p, cc, zz, xx):
        return VT.at[p, 0:HEAD_DIM, pl.ds(pl.multiple_of(slot(cc, zz, xx), LANES), HB)]

    for dx in range(1, X):
        to = dev(dx=dx)
        links.send(("g", dx), GS, GX.at[x], to)
        links.send(("k", dx), KS.at[xrel(dx)], k_block(c, z, x), to)
        for p in range(2):
            links.send(("v", p, dx), VS.at[xrel(dx), p], v_block(p, c, z, x), to)
    q_all = jnp.dot(rows, W[:, 0:WC], preferred_element_type=jnp.float32)
    q_all = q_all.astype(jnp.bfloat16).astype(jnp.float32) * (HEAD_DIM**-0.5 * LOG2E)
    q_all = q_all.T
    for h in range(X):
        QS[h] = q_all[h * HEAD_DIM : (h + 1) * HEAD_DIM].astype(jnp.bfloat16)
    for dx in range(1, X):
        links.send(("q", dx), QS.at[xrel(dx)], QT.at[x], dev(dx=dx))
    GX[x] = GS[...]
    k_block(c, z, x)[...] = KS[x]
    for p in range(2):
        v_block(p, c, z, x)[...] = VS[x, p]
    QT[x] = QS[x]

    QB[...] = jnp.zeros_like(QB)
    VT[:, HEAD_DIM:, :] = jnp.ones((2, VT.shape[1] - HEAD_DIM, VT.shape[2]), jnp.bfloat16)
    M[...] = jnp.full(M.shape, LOW, jnp.float32)
    ACC[...] = jnp.zeros_like(ACC)

    def my_row(block):
        row = lax.broadcasted_iota(jnp.int32, block.shape, 0)
        return row

    for dx in range(1, X):
        links.recv(("g", dx), GX.at[xrel(-dx)], dev(dx=-dx))
    row8 = lax.broadcasted_iota(jnp.int32, (8, GB), 0)
    own_gates = jnp.zeros((8, GB), jnp.float32)
    for sx in range(X):
        picked = jnp.sum(jnp.where(row8 == x, GX[sx], 0.0), axis=0, keepdims=True)
        own_gates = jnp.where(row8 == sx, picked, own_gates)
    GP[...] = own_gates
    links.send(("gp",), GP, GPR, dev(dc=1))

    for dx in range(1, X):
        sx = xrel(-dx)
        links.recv(("k", dx), k_block(c, z, sx), dev(dx=-dx))
        for p in range(2):
            links.recv(("v", p, dx), v_block(p, c, z, sx), dev(dx=-dx))

    def kv_views(cc, zz):
        at = pl.multiple_of(slot(cc, zz, 0), LANES)
        return [
            K.at[pl.ds(at, X * HB), :],
            VT.at[0, 0:HEAD_DIM, pl.ds(at, X * HB)],
            VT.at[1, 0:HEAD_DIM, pl.ds(at, X * HB)],
        ]

    def kv(zz, cc):
        return kv_views(cc, zz)

    ring_start("kv", kv)

    links.recv(("gp",), GPR, dev(dc=1))
    theirs = GPR[...]
    chip_gates = jnp.zeros((8, GB), jnp.float32)
    for sx in range(X):
        a, b = own_gates[sx : sx + 1], theirs[sx : sx + 1]
        chip_gates = jnp.where(row8 == 2 * sx, jnp.where(c == 0, a, b), chip_gates)
        chip_gates = jnp.where(row8 == 2 * sx + 1, jnp.where(c == 0, b, a), chip_gates)
    G[z] = chip_gates
    for d in range(1, Z):
        links.send(("gz", d), G.at[z], G.at[z], dev(dz=d))
    for dx in range(1, X):
        links.recv(("q", dx), QT.at[xrel(-dx)], dev(dx=-dx))
    for sx in range(X):
        QB[sx, 0:HEAD_DIM, 0:GB] = QT[sx]
        QB[sx, HEAD_DIM:, GB:] = QT[sx]
    for d in range(1, Z):
        links.recv(("woz", d), wo_block(c, x, zrel(-d), y), dev(dz=-d))
    for dx, dy in plane:
        own = wo_bundle(c, x, y)
        links.send(("woxy", dx, dy), own, own, dev(dx=dx, dy=dy))
    links.send(("woc", 0, 0), wo_bundle(c, x, y), wo_bundle(c, x, y), dev(dc=1))

    for d in range(1, Z):
        links.recv(("gz", d), G.at[zrel(-d)], dev(dz=-d))
    cum = G[...].reshape(Z * 8, GB)
    lane = lax.broadcasted_iota(jnp.int32, cum.shape, 1)
    step = 1
    while step < GB:
        cum = cum + jnp.where(lane >= step, pltpu.roll(cum, step, 1), 0.0)
        step *= 2
    total = jnp.broadcast_to(cum[:, GB - 1 :], (Z * 8, LANES))
    row = lax.broadcasted_iota(jnp.int32, total.shape, 0)
    before = jnp.where(row >= 1, pltpu.roll(total, 1, 0), 0.0)
    step = 1
    while step < Z * 8:
        before = before + jnp.where(row >= step, pltpu.roll(before, step, 0), 0.0)
        step *= 2
    cum = (cum + before[:, 0:1]) * LOG2E
    CUM[...] = cum.reshape(Z, 8, GB)

    cum_here = CUM[z]
    cum_q = [
        jnp.sum(jnp.where(row8 == 2 * sx + c, cum_here, 0.0), axis=0, keepdims=True)
        for sx in range(X)
    ]

    def key_bias(zz, cc):
        block = CUM[zz]
        block = jnp.where(cc == 0, block, pltpu.roll(block, 7, 0))
        both = jnp.concatenate([block[:, :HB], block[:, HB:]], axis=0)
        both = jnp.concatenate([both, jnp.zeros((LANES - 16, HB), jnp.float32)], axis=0)
        return both.T

    def chunk(bias, at, pair, tiles, mask):
        at = pl.multiple_of(at + pair * 2 * HB, 2 * HB)
        keys = K[pl.ds(at, 2 * HB), :]
        v0 = VT[0, :, pl.ds(at, 2 * HB)]
        v1 = VT[1, :, pl.ds(at, 2 * HB)]
        b0, b1 = bias
        for t in tiles:
            s = jnp.dot(keys, QB[t], preferred_element_type=jnp.float32)
            s0, s1 = s[:, :GB] - b0, s[:, GB:] - b1
            if mask is not None:
                s0, s1 = mask(s0, 0, t), mask(s1, 1, t)
            old = M[t]
            best = jnp.maximum(jnp.max(s0, axis=0, keepdims=True), jnp.max(s1, axis=0, keepdims=True))
            new = jnp.maximum(old, best + cum_q[t])
            rescale = jnp.exp2(old - new)
            shift = new - cum_q[t]
            p0 = jnp.exp2(s0 - shift).astype(jnp.bfloat16)
            p1 = jnp.exp2(s1 - shift).astype(jnp.bfloat16)
            M[t] = new
            ACC[t] = (
                ACC[t] * rescale
                + jnp.dot(v0, p0, preferred_element_type=jnp.float32)
                + jnp.dot(v1, p1, preferred_element_type=jnp.float32)
            )

    def columns(table, pair):
        even, odd = 4 * pair, 4 * pair + 2
        b0 = jnp.concatenate([table[:, even : even + 1], table[:, odd : odd + 1]], axis=0)
        b1 = jnp.concatenate([table[:, 8 + even : 9 + even], table[:, 8 + odd : 9 + odd]], axis=0)
        return b0, b1

    def past(zz, cc):
        table = key_bias(zz, cc)
        for pair in range(X // 2):
            chunk(columns(table, pair), slot(cc, zz, 0), pair, range(X), None)

    def present(cc):
        table = key_bias(z, cc)
        for pair in range(X // 2):

            def mask(s, which, t, pair=pair):
                r = lax.broadcasted_iota(jnp.int32, s.shape, 0)
                first = 2 * (2 * pair) + cc
                key = jnp.where(r < HB, first * GB + r, (first + 2) * GB + r - HB) + which * HB
                query = (2 * t + c) * GB + lax.broadcasted_iota(jnp.int32, s.shape, 1)
                return jnp.where(key <= query, s, LOW)

            full = [t for t in range(X) if t > 2 * pair + 1]
            cut = [t for t in range(X) if 2 * pair <= t <= 2 * pair + 1]
            bias = columns(table, pair)
            chunk(bias, slot(cc, z, 0), pair, cut, mask)
            if full:
                chunk(bias, slot(cc, z, 0), pair, full, None)

    present_own = functools.partial(present, c)

    def both_cores(zz):
        @pl.loop(0, 2)
        def _(i):
            past(zz, jnp.where(i == 0, c, co))

    present_own()
    other_core("kv", kv, 0)
    present(co)
    for k in range(1, UP + 1):
        ring_step("kv", kv, k)
        other_core("kv", kv, -k)
        if k <= DN:
            other_core("kv", kv, k)

        @pl.when(z - k >= 0)
        def _():
            both_cores(zrel(-k))

        if k <= DN:

            @pl.when(z + k >= Z)
            def _():
                both_cores(zrel(k))

    for dx, dy in plane:
        theirs = wo_bundle(c, xrel(-dx), yrel(-dy))
        links.recv(("woxy", dx, dy), theirs, dev(dx=-dx, dy=-dy))
        links.send(("woc", dx, dy), theirs, theirs, dev(dc=1))

    for t in range(X):
        acc = ACC[t]
        o = (acc[:HEAD_DIM] / acc[HEAD_DIM : HEAD_DIM + 1]).astype(jnp.bfloat16)
        for yy in range(Y):
            OS[t, yy, :, 0:TB] = o[:, yy * TB : (yy + 1) * TB]

    def at_rows(xx, yy):
        return AT.at[pl.ds(pl.multiple_of((yy * X + xx) * HEAD_DIM, HEAD_DIM), HEAD_DIM), :]

    for dx, dy in plane:
        links.send(("o", dx, dy), OS.at[xrel(dx), yrel(dy)], at_rows(x, y), dev(dx=dx, dy=dy))
    at_rows(x, y)[...] = OS[x, y]
    for dx in range(X):
        for dy in range(Y):
            theirs = wo_bundle(co, xrel(-dx), yrel(-dy))
            links.recv(("woc", dx, dy), theirs, dev(dc=1))
    for dx, dy in plane:
        links.recv(("o", dx, dy), at_rows(xrel(-dx), yrel(-dy)), dev(dx=-dx, dy=-dy))

    attended = AT[...]
    for cc in range(C):
        for xx in range(X):
            block = (cc * X + xx) * Z * PR
            part = jnp.dot(
                WO[block : block + Z * PR, :], attended, preferred_element_type=jnp.float32
            )
            for zz in range(Z):
                to = ((zz * X + xx) * C + cc) * PR
                PT[to : to + PR, :] = part[zz * PR : (zz + 1) * PR]
    out_ref[...] = rms_norm(PT[...].T[:TB], ogain_ref[...])
    links.drain()


def layer(dims, tokens, norm_gain, w_query, w_key, w_value, w_forget, forget_offset, w_out_t, out_gain):
    Z, X, C, Y = dims
    TB, D = tokens.shape
    PR, WC = w_query.shape
    GB = TB * Y
    HB = GB // 2
    LW = -(-(3 * WC + LANES) // (2 * LANES)) * 2 * LANES
    pad = jnp.zeros((PR, LW - 3 * WC - w_forget.shape[1]), jnp.bfloat16)
    wcat = jnp.concatenate([w_query, w_key, w_value, w_forget, pad], axis=1)
    keys = Z * X * C * HB
    UP = Z // 2
    n_sems = (
        X * C + Y + 4 * Z + 2 * Z * 3 + 2 * Z * 3 + 6 * X + 2 * Z + 3 * X * Y + 16
    )
    vmem, smem = pl.BlockSpec(memory_space=pltpu.VMEM), pl.BlockSpec(memory_space=pltpu.SMEM)
    bf16, f32 = jnp.bfloat16, jnp.float32
    scratch = [
        pltpu.VMEM((D, LW), bf16),
        pltpu.VMEM((GB, D), bf16),
        pltpu.VMEM((D, D), bf16),
        pltpu.VMEM((X, HB, LANES), bf16),
        pltpu.VMEM((X, 2, HEAD_DIM, HB), bf16),
        pltpu.VMEM((X, HEAD_DIM, GB), bf16),
        pltpu.VMEM((8, GB), f32),
        pltpu.VMEM((X, 8, GB), f32),
        pltpu.VMEM((8, GB), f32),
        pltpu.VMEM((8, GB), f32),
        pltpu.VMEM((Z, 8, GB), f32),
        pltpu.VMEM((Z, 8, GB), f32),
        pltpu.VMEM((keys, LANES), bf16),
        pltpu.VMEM((2, HEAD_DIM + 16, keys), bf16),
        pltpu.VMEM((X, HEAD_DIM, GB), bf16),
        pltpu.VMEM((X, LANES, 2 * GB), bf16),
        pltpu.VMEM((X, 1, GB), f32),
        pltpu.VMEM((X, HEAD_DIM + 16, GB), f32),
        pltpu.VMEM((X, Y, HEAD_DIM, LANES), bf16),
        pltpu.VMEM((D, LANES), bf16),
        pltpu.VMEM((D, LANES), f32),
        pltpu.SemaphoreType.DMA((n_sems,)),
        pltpu.SemaphoreType.DMA((n_sems,)),
    ]
    return pl.pallas_call(
        functools.partial(kernel, dims),
        out_shape=jax.ShapeDtypeStruct((TB, D), bf16),
        in_specs=[vmem, vmem, vmem, smem, vmem, vmem],
        out_specs=vmem,
        scratch_shapes=scratch,
        compiler_params=pltpu.CompilerParams(
            collective_id=0, has_side_effects=True, vmem_limit_bytes=56 * 1024 * 1024
        ),
    )(tokens, norm_gain.reshape(1, D), wcat, forget_offset, w_out_t, out_gain.reshape(1, D))


def sharded(mesh, dims):
    finer = Mesh(mesh.devices.reshape(*dims), AXES)
    sp = ("z", "x", "c")
    return jax.shard_map(
        functools.partial(layer, dims),
        mesh=finer,
        in_specs=(
            P(AXES, None),
            P(),
            P(sp, "y"),
            P(sp, "y"),
            P(sp, "y"),
            P(sp, "y"),
            P("y"),
            P(sp, "y"),
            P(),
        ),
        out_specs=P(AXES, None),
        check_vma=False,
    )


def solution(mesh):
    return sharded(mesh, (8, 4, 2, mesh.shape["tp"]))
```

```python
import functools
import math

import jax
import jax.numpy as jnp
from jax import lax
from jax.experimental import pallas as pl
from jax.experimental.pallas import tpu as pltpu
from jax.sharding import Mesh
from jax.sharding import PartitionSpec as P

HEAD_DIM = 64
AXES = ("z", "x", "c", "y")
MESH = pl.DeviceIdType.MESH
EPS = 1e-06
LOG2E = 1.4426950408889634
LOW = -1e30
LANES = 128


def rms_norm(floats, gain_row):
    scale_row = lax.rsqrt(jnp.mean(floats * floats, axis=-1, keepdims=True) + EPS)
    return (floats * scale_row * gain_row).astype(jnp.bfloat16)


def log_sigmoid(t):
    u = jnp.exp(-jnp.abs(t))
    series = u * (1.0 - u * (0.5 - u * (1.0 / 3.0 - u * 0.25)))
    return jnp.minimum(t, 0.0) - jnp.where(u < 0.01, series, jnp.log(1.0 + u))


class Links:
    def __init__(self, send_sems, recv_sems, ids):
        self.send_sems, self.recv_sems, self.ids, self.sent = send_sems, recv_sems, ids, []

    def copy(self, key, src, dst, dev):
        at = self.ids.setdefault(key, len(self.ids))
        return pltpu.make_async_remote_copy(
            src_ref=src,
            dst_ref=dst,
            send_sem=self.send_sems.at[at],
            recv_sem=self.recv_sems.at[at],
            device_id=dev,
            device_id_type=MESH,
        )

    def send(self, key, src, dst, dev):
        c = self.copy(key, src, dst, dev)
        c.start()
        self.sent.append(c)

    def recv(self, key, landed, dev):
        self.copy(key, landed, landed, dev).wait_recv()

    def drain(self):
        for c in self.sent:
            c.wait_send()


def kernel(
    dims,
    tokens_ref,
    gain_ref,
    wq_ref,
    wk_ref,
    wv_ref,
    wf_ref,
    off_ref,
    wo_ref,
    ogain_ref,
    out_ref,
    W,
    XN,
    WO,
    KS,
    VS,
    QS,
    GS,
    GX,
    GP,
    GPR,
    G,
    CUM,
    K,
    VT,
    QT,
    QB,
    M,
    ACC,
    OS,
    AT,
    PT,
    SC,
    PB,
    send_sems,
    recv_sems,
):
    Z, X, C, Y = dims
    TB, D = tokens_ref.shape
    GB = TB * Y
    HB = GB // 2
    PR, WC = wo_ref.shape
    LW = W.shape[2]
    z, x, c, y = (lax.axis_index(a) for a in AXES)
    links = Links(send_sems, recv_sems, {})

    def dev(dz=0, dx=0, dc=0, dy=0):
        return {
            "z": lax.rem(z + (dz % Z), Z),
            "x": lax.rem(x + (dx % X), X),
            "c": lax.rem(c + (dc % C), C),
            "y": lax.rem(y + (dy % Y), Y),
        }

    def zrel(d):
        return lax.rem(z + (d % Z), Z)

    def xrel(d):
        return lax.rem(x + (d % X), X)

    def yrel(d):
        return lax.rem(y + (d % Y), Y)

    co = 1 - c
    plane = [(dx, dy) for dx in range(X) for dy in range(Y) if (dx, dy) != (0, 0)]
    far_first = sorted(range(1, Z), key=lambda d: -min(d, Z - d))
    near_first = [0] + far_first[::-1]
    x_near, y_near = ([1] if n == 2 else [1, -1] for n in (X, Y))

    barrier = pltpu.get_barrier_semaphore()
    greeted = (
        [dict(dx=dx, dy=dy) for dx, dy in plane] + [dict(dc=1)] + [dict(dz=d) for d in range(1, Z)]
    )
    for g in greeted:
        pl.semaphore_signal(barrier, inc=1, device_id=dev(**g), device_id_type=MESH)

    def w_rows(xx, cc):
        return pl.ds(pl.multiple_of((xx * C + cc) * PR, PR), PR)

    KV, QF = (0, 2 * WC), (2 * WC, LW)
    mine = w_rows(x, c)
    W[z, mine, 0:WC] = wk_ref[...]
    W[z, mine, WC : 2 * WC] = wv_ref[...]
    W[z, mine, 2 * WC : 3 * WC] = wq_ref[...]
    W[z, mine, 3 * WC :] = jnp.zeros((PR, LANES), jnp.bfloat16)
    W[z, mine, 3 * WC : 3 * WC + wf_ref.shape[1]] = wf_ref[...]

    def t_rows(yy, lo=0, count=TB):
        return XN.at[pl.ds(pl.multiple_of(yy * TB + lo, 32), count), :]

    t_rows(y)[...] = rms_norm(tokens_ref[...].astype(jnp.float32), gain_ref[...])

    def wo_block(cc, xx, zz, yy):
        row = ((cc * X + xx) * Z + zz) * PR
        return WO.at[
            pl.ds(pl.multiple_of(row, PR), PR), pl.ds(pl.multiple_of(yy * WC, LANES), WC)
        ]

    def wo_bundle(cc, xx, yy):
        row = (cc * X + xx) * Z * PR
        return WO.at[
            pl.ds(pl.multiple_of(row, PR), Z * PR), pl.ds(pl.multiple_of(yy * WC, LANES), WC)
        ]

    wo_block(c, x, z, y)[...] = wo_ref[...]
    pl.semaphore_wait(barrier, len(greeted))

    def w_unit(d, xx, cc, lanes):
        return W.at[zrel(d), w_rows(xx, cc), lanes[0] : lanes[1]]

    def w_bundle(xx, cc, lanes):
        return W.at[:, w_rows(xx, cc), lanes[0] : lanes[1]]

    def halves(lanes):
        middle = lanes[0] + WC
        return (lanes[0], middle), (middle, lanes[1])

    def along_x(d, lanes):
        for dx in x_near:
            unit = w_unit(d, x, c, lanes)
            links.send(("x1", lanes, d, dx), unit, unit, dev(dx=dx))

    def z_stage(lanes):
        for d in near_first:
            if d != 0:
                links.recv(("wz", lanes, d), w_unit(-d, x, c, lanes), dev(dz=-d))
            along_x(-d % Z, lanes)
        own = w_bundle(x, c, lanes)
        links.send(("wc", lanes, 0), own, own, dev(dc=1))

    def x_stage(lanes):
        for d in near_first:
            for dx, part in zip(x_near, halves(lanes)):
                links.recv(("x1", lanes, -d % Z, dx), w_unit(-d, xrel(-dx), c, lanes), dev(dx=-dx))
                if X > 2:
                    unit = w_unit(-d, xrel(-dx), c, part)
                    links.send(("x2", lanes, -d % Z, dx), unit, unit, dev(dx=dx))
        for dx in x_near:
            theirs = w_bundle(xrel(-dx), c, lanes)
            links.send(("wc", lanes, dx % X), theirs, theirs, dev(dc=1))

    def x_last(lanes):
        if X > 2:
            for d in near_first:
                for dx, part in zip(x_near, halves(lanes)):
                    unit = w_unit(-d, xrel(2), c, part)
                    links.recv(("x2", lanes, -d % Z, dx), unit, dev(dx=-dx))
            theirs = w_bundle(xrel(2), c, lanes)
            links.send(("wc", lanes, 2), theirs, theirs, dev(dc=1))

    def core_last(lanes):
        for dx in range(X):
            links.recv(("wc", lanes, dx), w_bundle(xrel(-dx), co, lanes), dev(dc=1))

    for lanes in (KV, QF):
        for d in far_first:
            unit = w_unit(0, x, c, lanes)
            links.send(("wz", lanes, d), unit, unit, dev(dz=d))
    for dy in y_near:
        links.send(("tok", dy), t_rows(y), t_rows(y), dev(dy=dy))
    for d in far_first:
        links.send(("woz", d), wo_ref, wo_block(c, x, z, y), dev(dz=d))

    QB[...] = jnp.zeros_like(QB)
    VT[:, HEAD_DIM:, :] = jnp.ones((2, VT.shape[1] - HEAD_DIM, VT.shape[2]), jnp.bfloat16)
    M[...] = jnp.full(M.shape, LOW, jnp.float32)
    ACC[...] = jnp.zeros_like(ACC)

    z_stage(KV)
    for dy, lo in zip(y_near, (0, TB // 2)):
        links.recv(("tok", dy), t_rows(yrel(-dy)), dev(dy=-dy))
        if Y > 2:
            part = t_rows(yrel(-dy), lo, TB // 2)
            links.send(("tok2", dy), part, part, dev(dy=dy))
    x_stage(KV)
    z_stage(QF)
    x_last(KV)
    x_stage(QF)
    if Y > 2:
        for dy, lo in zip(y_near, (0, TB // 2)):
            links.recv(("tok2", dy), t_rows(yrel(2), lo, TB // 2), dev(dy=-dy))
    core_last(KV)

    rows = XN[...]

    def project(lo, count):
        weight = W[:, :, lo : lo + count].reshape(D, count)
        return jnp.dot(rows, weight, preferred_element_type=jnp.float32)

    def slot(cc, zz, xx):
        return ((cc * Z + zz) * X + xx) * HB

    def k_block(cc, zz, xx):
        return K.at[pl.ds(pl.multiple_of(slot(cc, zz, xx), LANES), HB), :]

    def v_block(p, cc, zz, xx):
        return VT.at[p, 0:HEAD_DIM, pl.ds(pl.multiple_of(slot(cc, zz, xx), LANES), HB)]

    k_all = project(0, WC)
    for h in range(X):
        kh = k_all[:, h * HEAD_DIM : (h + 1) * HEAD_DIM]
        KS[h] = jnp.concatenate([kh[:HB], kh[HB:]], axis=1).astype(jnp.bfloat16)
    for dx in range(1, X):
        links.send(("k", dx), KS.at[xrel(dx)], k_block(c, z, x), dev(dx=dx))
    v_all = project(WC, WC).T
    for h in range(X):
        vh = v_all[h * HEAD_DIM : (h + 1) * HEAD_DIM].astype(jnp.bfloat16)
        VS[h, 0] = vh[:, :HB]
        VS[h, 1] = vh[:, HB:]
    for dx in range(1, X):
        for p in range(2):
            links.send(("v", p, dx), VS.at[xrel(dx), p], v_block(p, c, z, x), dev(dx=dx))
    k_block(c, z, x)[...] = KS[x]
    for p in range(2):
        v_block(p, c, z, x)[...] = VS[x, p]

    x_last(QF)
    core_last(QF)
    gates = project(3 * WC, LANES).T[:8]
    head_row = lax.broadcasted_iota(jnp.int32, gates.shape, 0)
    offset = jnp.zeros_like(gates)
    for h in range(X):
        offset = jnp.where(head_row == h, off_ref[h], offset)
    GS[...] = log_sigmoid(gates + offset + math.log(GB * Z * X * C))
    for dx in range(1, X):
        links.send(("g", dx), GS, GX.at[x], dev(dx=dx))
    q_all = project(2 * WC, WC)
    q_all = q_all.astype(jnp.bfloat16).astype(jnp.float32) * (HEAD_DIM**-0.5 * LOG2E)
    q_all = q_all.T
    for h in range(X):
        QS[h] = q_all[h * HEAD_DIM : (h + 1) * HEAD_DIM].astype(jnp.bfloat16)
    for dx in range(1, X):
        links.send(("q", dx), QS.at[xrel(dx)], QT.at[x], dev(dx=dx))
    GX[x] = GS[...]
    QT[x] = QS[x]

    UP = DN = Z // 2

    def goes(way, a, k):
        return k < UP or (k == UP and (a == 0) == (way == "up"))

    def kv(zz, cc):
        at = pl.multiple_of(slot(cc, zz, 0), LANES)
        return [
            K.at[pl.ds(at, X * HB), :],
            VT.at[0, 0:HEAD_DIM, pl.ds(at, X * HB)],
            VT.at[1, 0:HEAD_DIM, pl.ds(at, X * HB)],
        ]

    WAYS = (("up", 1), ("dn", -1))

    def ring_start():
        for a, view in enumerate(kv(z, c)):
            for way, sign in WAYS:
                if goes(way, a, 1):
                    links.send((way, 1, a), view, view, dev(dz=sign))
        for a, view in enumerate(kv(z, c)):
            links.send(("core", 0, a), view, view, dev(dc=1))

    def ring_step(k):
        for a in range(3):
            for way, sign in WAYS:
                if goes(way, a, k):
                    view = kv(zrel(-sign * k), c)[a]
                    links.recv((way, k, a), view, dev(dz=-sign))
                    if goes(way, a, k + 1):
                        links.send((way, k + 1, a), view, view, dev(dz=sign))
                    links.send(("core", -sign * k % Z, a), view, view, dev(dc=1))

    def other_core(d):
        for a, view in enumerate(kv(zrel(d), co)):
            links.recv(("core", d % Z, a), view, dev(dc=1))

    for dx in range(1, X):
        sx = xrel(-dx)
        links.recv(("k", dx), k_block(c, z, sx), dev(dx=-dx))
        for p in range(2):
            links.recv(("v", p, dx), v_block(p, c, z, sx), dev(dx=-dx))
    ring_start()

    for dx in range(1, X):
        links.recv(("g", dx), GX.at[xrel(-dx)], dev(dx=-dx))
    row8 = lax.broadcasted_iota(jnp.int32, (8, GB), 0)
    own_gates = jnp.zeros((8, GB), jnp.float32)
    for sx in range(X):
        picked = jnp.sum(jnp.where(row8 == x, GX[sx], 0.0), axis=0, keepdims=True)
        own_gates = jnp.where(row8 == sx, picked, own_gates)
    GP[...] = own_gates
    links.send(("gp",), GP, GPR, dev(dc=1))
    links.recv(("gp",), GPR, dev(dc=1))
    theirs = GPR[...]
    chip_gates = jnp.zeros((8, GB), jnp.float32)
    for sx in range(X):
        a, b = own_gates[sx : sx + 1], theirs[sx : sx + 1]
        chip_gates = jnp.where(row8 == 2 * sx, jnp.where(c == 0, a, b), chip_gates)
        chip_gates = jnp.where(row8 == 2 * sx + 1, jnp.where(c == 0, b, a), chip_gates)
    G[z] = chip_gates
    for d in far_first:
        links.send(("gz", d), G.at[z], G.at[z], dev(dz=d))
    for dx in range(1, X):
        links.recv(("q", dx), QT.at[xrel(-dx)], dev(dx=-dx))
    for sx in range(X):
        QB[sx, 0:HEAD_DIM, 0:GB] = QT[sx]
        QB[sx, HEAD_DIM:, GB:] = QT[sx]
    for d in far_first:
        links.recv(("woz", d), wo_block(c, x, zrel(-d), y), dev(dz=-d))
    own = wo_bundle(c, x, y)
    for dx, dy in plane:
        links.send(("woxy", dx, dy), own, own, dev(dx=dx, dy=dy))
    links.send(("woc", 0, 0), own, own, dev(dc=1))

    def cumulative(block):
        n = block.shape[0]
        lane = lax.broadcasted_iota(jnp.int32, block.shape, 1)
        step = 1
        while step < GB:
            block = block + jnp.where(lane >= step, pltpu.roll(block, step, 1), 0.0)
            step *= 2
        total = jnp.broadcast_to(block[:, GB - 1 :], (n, LANES))
        row = lax.broadcasted_iota(jnp.int32, total.shape, 0)
        before = jnp.where(row >= 1, pltpu.roll(total, 1, 0), 0.0)
        step = 1
        while step < n:
            before = before + jnp.where(row >= step, pltpu.roll(before, step, 0), 0.0)
            step *= 2
        return (block + before[:, 0:1]) * LOG2E

    def query_sums(block):
        return [
            jnp.sum(jnp.where(row8 == 2 * sx + c, block, 0.0), axis=0, keepdims=True)
            for sx in range(X)
        ]

    def key_sums(block, cc):
        block = jnp.where(cc == 0, block, pltpu.roll(block, 7, 0))
        both = jnp.concatenate([block[:, :HB], block[:, HB:]], axis=0)
        both = jnp.concatenate([both, jnp.zeros((LANES - 16, HB), jnp.float32)], axis=0)
        return both.T

    def attend(items, cum_q):
        AHEAD, SOFT = 3, 1
        n_s, n_p = AHEAD - SOFT + 1, SOFT + 1
        best, rescale, loaded = {}, {}, {}

        def prepared(table, at, pair):
            key = (id(table), pair)
            if key not in loaded:
                even, odd = 4 * pair, 4 * pair + 2
                b0 = [table[:, even : even + 1], table[:, odd : odd + 1]]
                b1 = [table[:, 8 + even : 9 + even], table[:, 8 + odd : 9 + odd]]
                start = pl.multiple_of(at + pair * 2 * HB, 2 * HB)
                loaded[key] = jnp.concatenate(b0, axis=0), jnp.concatenate(b1, axis=0), start
            return loaded[key]

        def scores(j):
            table, at, pair, t, mask = items[j]
            b0, b1, start = prepared(table, at, pair)
            s = jnp.dot(K[pl.ds(start, 2 * HB), :], QB[t], preferred_element_type=jnp.float32)
            s0, s1 = s[:, :GB] - b0, s[:, GB:] - b1
            if mask is not None:
                s0, s1 = mask(s0, 0, t), mask(s1, 1, t)
            SC[j % n_s, 0], SC[j % n_s, 1] = s0, s1
            best[j] = jnp.maximum(jnp.max(s0, axis=0, keepdims=True), jnp.max(s1, axis=0, keepdims=True))

        def softmax(j):
            t = items[j][3]
            old = M[t]
            new = jnp.maximum(old, best[j] + cum_q[t])
            rescale[j] = jnp.exp2(old - new)
            M[t] = new
            shift = new - cum_q[t]
            PB[j % n_p, : 2 * HB] = jnp.exp2(SC[j % n_s, 0] - shift).astype(jnp.bfloat16)
            PB[j % n_p, 2 * HB :] = jnp.exp2(SC[j % n_s, 1] - shift).astype(jnp.bfloat16)

        def weigh(j):
            table, at, pair, t, _ = items[j]
            start = prepared(table, at, pair)[2]
            v = jnp.concatenate(
                [VT[0, :, pl.ds(start, 2 * HB)], VT[1, :, pl.ds(start, 2 * HB)]], axis=1
            )
            ACC[t] = ACC[t] * rescale[j] + jnp.dot(
                v, PB[j % n_p], preferred_element_type=jnp.float32
            )

        for j in range(-AHEAD, len(items)):
            if 0 <= j + AHEAD < len(items):
                scores(j + AHEAD)
            if j >= 0:
                weigh(j)
            if 0 <= j + SOFT < len(items):
                softmax(j + SOFT)

    cum_here = cumulative(G[z])
    cum_q_here = query_sums(cum_here)

    @pl.loop(0, 2)
    def _(i):
        cc = jnp.where(i == 0, c, co)

        @pl.when(i == 1)
        def _():
            other_core(0)

        def masked(pair):
            def mask(s, which, t):
                r = lax.broadcasted_iota(jnp.int32, s.shape, 0)
                first = 4 * pair + cc
                key = jnp.where(r < HB, first * GB + r, (first + 2) * GB + r - HB) + which * HB
                query = (2 * t + c) * GB + lax.broadcasted_iota(jnp.int32, s.shape, 1)
                return jnp.where(key <= query, s, LOW)

            return mask

        table = key_sums(cum_here, cc)
        items = [
            (table, slot(cc, z, 0), pair, t, masked(pair) if t <= 2 * pair + 1 else None)
            for pair in range(X // 2)
            for t in range(2 * pair, X)
        ]
        attend(items, cum_q_here)

    for d in far_first:
        links.recv(("gz", d), G.at[zrel(-d)], dev(dz=-d))
    CUM[...] = cumulative(G[...].reshape(Z * 8, GB)).reshape(Z, 8, GB)
    cum_q = query_sums(CUM[z])

    def past(ds):
        @pl.loop(0, 2)
        def _(i):
            cc = jnp.where(i == 0, c, co)

            @pl.when(i == 1)
            def _():
                for d in ds:
                    other_core(d)

            items = []
            for d in ds:
                zz = zrel(d)
                table = key_sums(CUM[zz], cc)
                items += [
                    (table, slot(cc, zz, 0), pair, t, None)
                    for pair in range(X // 2)
                    for t in range(X)
                ]
            attend(items, cum_q)

    def skipped(ds):
        for d in ds:
            other_core(d)

    def wo_forward():
        for dx, dy in plane:
            theirs = wo_bundle(c, xrel(-dx), yrel(-dy))
            links.recv(("woxy", dx, dy), theirs, dev(dx=-dx, dy=-dy))
            links.send(("woc", dx, dy), theirs, theirs, dev(dc=1))

    for k in range(1, UP + 1):
        ring_step(k)
        if k == UP:
            wo_forward()
        both = [-k, k] if k < UP else [-k]
        if k < UP:

            @pl.when(z + k >= Z)
            def _():
                past(both)

            @pl.when((z >= k) & (z + k < Z))
            def _():
                past([-k])
                skipped([k])

        else:

            @pl.when(z >= k)
            def _():
                past(both)

        @pl.when(z < k)
        def _():
            skipped(both)

    for t in range(X):
        acc = ACC[t]
        o = (acc[:HEAD_DIM] / acc[HEAD_DIM : HEAD_DIM + 1]).astype(jnp.bfloat16)
        for yy in range(Y):
            OS[t, yy, :, 0:TB] = o[:, yy * TB : (yy + 1) * TB]

    def at_rows(xx, yy):
        return AT.at[pl.ds(pl.multiple_of((yy * X + xx) * HEAD_DIM, HEAD_DIM), HEAD_DIM), :]

    for dx, dy in plane:
        links.send(("o", dx, dy), OS.at[xrel(dx), yrel(dy)], at_rows(x, y), dev(dx=dx, dy=dy))
    at_rows(x, y)[...] = OS[x, y]
    for dx in range(X):
        for dy in range(Y):
            theirs = wo_bundle(co, xrel(-dx), yrel(-dy))
            links.recv(("woc", dx, dy), theirs, dev(dc=1))
    for dx, dy in plane:
        links.recv(("o", dx, dy), at_rows(xrel(-dx), yrel(-dy)), dev(dx=-dx, dy=-dy))

    attended = AT[...]
    for cc in range(C):
        for xx in range(X):
            block = (cc * X + xx) * Z * PR
            part = jnp.dot(
                WO[block : block + Z * PR, :], attended, preferred_element_type=jnp.float32
            )
            for zz in range(Z):
                to = ((zz * X + xx) * C + cc) * PR
                PT[to : to + PR, :] = part[zz * PR : (zz + 1) * PR]
    out_ref[...] = rms_norm(PT[...].T[:TB], ogain_ref[...])
    links.drain()


def layer(dims, tokens, norm_gain, w_query, w_key, w_value, w_forget, forget_offset, w_out_t, out_gain):
    Z, X, C, Y = dims
    TB, D = tokens.shape
    PR, WC = w_query.shape
    GB = TB * Y
    HB = GB // 2
    LW = 3 * WC + LANES
    keys = Z * X * C * HB
    n_sems = 260
    vmem, smem = pl.BlockSpec(memory_space=pltpu.VMEM), pl.BlockSpec(memory_space=pltpu.SMEM)
    bf16, f32 = jnp.bfloat16, jnp.float32
    scratch = [
        pltpu.VMEM((Z, X * C * PR, LW), bf16),
        pltpu.VMEM((GB, D), bf16),
        pltpu.VMEM((D, D), bf16),
        pltpu.VMEM((X, HB, LANES), bf16),
        pltpu.VMEM((X, 2, HEAD_DIM, HB), bf16),
        pltpu.VMEM((X, HEAD_DIM, GB), bf16),
        pltpu.VMEM((8, GB), f32),
        pltpu.VMEM((X, 8, GB), f32),
        pltpu.VMEM((8, GB), f32),
        pltpu.VMEM((8, GB), f32),
        pltpu.VMEM((Z, 8, GB), f32),
        pltpu.VMEM((Z, 8, GB), f32),
        pltpu.VMEM((keys, LANES), bf16),
        pltpu.VMEM((2, HEAD_DIM + 16, keys), bf16),
        pltpu.VMEM((X, HEAD_DIM, GB), bf16),
        pltpu.VMEM((X, LANES, 2 * GB), bf16),
        pltpu.VMEM((X, 1, GB), f32),
        pltpu.VMEM((X, HEAD_DIM + 16, GB), f32),
        pltpu.VMEM((X, Y, HEAD_DIM, LANES), bf16),
        pltpu.VMEM((D, LANES), bf16),
        pltpu.VMEM((D, LANES), f32),
        pltpu.VMEM((3, 2, 2 * HB, GB), f32),
        pltpu.VMEM((2, 4 * HB, GB), bf16),
        pltpu.SemaphoreType.DMA((n_sems,)),
        pltpu.SemaphoreType.DMA((n_sems,)),
    ]
    return pl.pallas_call(
        functools.partial(kernel, dims),
        out_shape=jax.ShapeDtypeStruct((TB, D), bf16),
        in_specs=[vmem] * 6 + [smem, vmem, vmem],
        out_specs=vmem,
        scratch_shapes=scratch,
        compiler_params=pltpu.CompilerParams(
            collective_id=0, has_side_effects=True, vmem_limit_bytes=56 * 1024 * 1024
        ),
    )(
        tokens,
        norm_gain.reshape(1, D),
        w_query,
        w_key,
        w_value,
        w_forget,
        forget_offset,
        w_out_t,
        out_gain.reshape(1, D),
    )


def sharded(mesh, dims):
    finer = Mesh(mesh.devices.reshape(*dims), AXES)
    sp = ("z", "x", "c")
    return jax.shard_map(
        functools.partial(layer, dims),
        mesh=finer,
        in_specs=(
            P(AXES, None),
            P(),
            P(sp, "y"),
            P(sp, "y"),
            P(sp, "y"),
            P(sp, "y"),
            P("y"),
            P(sp, "y"),
            P(),
        ),
        out_specs=P(AXES, None),
        check_vma=False,
    )


def solution(mesh):
    return sharded(mesh, (8, 4, 2, mesh.shape["tp"]))
```

```python
import functools
import math

import jax
import jax.numpy as jnp
from jax import lax
from jax.experimental import pallas as pl
from jax.experimental.pallas import tpu as pltpu
from jax.sharding import Mesh
from jax.sharding import PartitionSpec as P

HEAD_DIM = 64
AXES = ("z", "x", "c", "y")
MESH = pl.DeviceIdType.MESH
EPS = 1e-06
LOG2E = 1.4426950408889634
LOW = -1e30
LANES = 128


def rms_norm(floats, gain_row):
    scale_row = lax.rsqrt(jnp.mean(floats * floats, axis=-1, keepdims=True) + EPS)
    return (floats * scale_row * gain_row).astype(jnp.bfloat16)


def log_sigmoid(t):
    u = jnp.exp(-jnp.abs(t))
    series = u * (1.0 - u * (0.5 - u * (1.0 / 3.0 - u * 0.25)))
    return jnp.minimum(t, 0.0) - jnp.where(u < 0.01, series, jnp.log(1.0 + u))


class Links:
    def __init__(self, send_sems, recv_sems, ids):
        self.send_sems, self.recv_sems, self.ids, self.sent = send_sems, recv_sems, ids, []

    def copy(self, key, src, dst, dev):
        at = self.ids.setdefault(key, len(self.ids))
        return pltpu.make_async_remote_copy(
            src_ref=src,
            dst_ref=dst,
            send_sem=self.send_sems.at[at],
            recv_sem=self.recv_sems.at[at],
            device_id=dev,
            device_id_type=MESH,
        )

    def send(self, key, src, dst, dev):
        c = self.copy(key, src, dst, dev)
        c.start()
        self.sent.append(c)

    def recv(self, key, landed, dev):
        self.copy(key, landed, landed, dev).wait_recv()

    def drain(self):
        for c in self.sent:
            c.wait_send()


def kernel(
    dims,
    tokens_ref,
    gain_ref,
    wq_ref,
    wk_ref,
    wv_ref,
    wf_ref,
    off_ref,
    wo_ref,
    ogain_ref,
    out_ref,
    W,
    XN,
    WO,
    KS,
    VS,
    QS,
    GS,
    GX,
    GP,
    GPR,
    G,
    CUM,
    K,
    VT,
    QT,
    QB,
    M,
    ACC,
    OS,
    AT,
    PT,
    SC,
    PB,
    WO_OWN,
    send_sems,
    recv_sems,
):
    Z, X, C, Y = dims
    TB, D = tokens_ref.shape
    GB = TB * Y
    HB = GB // 2
    PR, WC = wo_ref.shape
    LW = W.shape[2]
    z, x, c, y = (lax.axis_index(a) for a in AXES)
    links = Links(send_sems, recv_sems, {})

    def dev(dz=0, dx=0, dc=0, dy=0):
        return {
            "z": lax.rem(z + (dz % Z), Z),
            "x": lax.rem(x + (dx % X), X),
            "c": lax.rem(c + (dc % C), C),
            "y": lax.rem(y + (dy % Y), Y),
        }

    def zrel(d):
        return lax.rem(z + (d % Z), Z)

    def xrel(d):
        return lax.rem(x + (d % X), X)

    def yrel(d):
        return lax.rem(y + (d % Y), Y)

    co = 1 - c
    plane = [(dx, dy) for dx in range(X) for dy in range(Y) if (dx, dy) != (0, 0)]
    far_first = sorted(range(1, Z), key=lambda d: -min(d, Z - d))
    near_first = [0] + far_first[::-1]
    x_near, y_near = ([1] if n == 2 else [1, -1] for n in (X, Y))

    barrier = pltpu.get_barrier_semaphore()
    greeted = (
        [dict(dx=dx, dy=dy) for dx, dy in plane] + [dict(dc=1)] + [dict(dz=d) for d in range(1, Z)]
    )
    for g in greeted:
        pl.semaphore_signal(barrier, inc=1, device_id=dev(**g), device_id_type=MESH)

    def w_rows(xx, cc):
        return pl.ds(pl.multiple_of((xx * C + cc) * PR, PR), PR)

    KVF, Q = (0, 2 * WC + LANES), (2 * WC + LANES, LW)
    mine = w_rows(x, c)
    W[z, mine, 0:WC] = wk_ref[...]
    W[z, mine, WC : 2 * WC] = wv_ref[...]
    W[z, mine, KVF[1] :] = wq_ref[...]
    PT[0:LANES] = jnp.zeros((LANES, LANES), jnp.float32)
    PT[0:X, 0:PR] = wf_ref[...].astype(jnp.float32)
    W[z, mine, 2 * WC : KVF[1]] = PT[0:LANES].T[:PR].astype(jnp.bfloat16)

    def t_rows(yy, lo=0, count=TB):
        return XN.at[pl.ds(pl.multiple_of(yy * TB + lo, 32), count), :]

    t_rows(y)[...] = rms_norm(tokens_ref[...].astype(jnp.float32), gain_ref[...])

    HALF = HEAD_DIM // 2
    WH = WC // 2

    def wo_columns(yy):
        return pl.ds(pl.multiple_of(yy * WH, WH), WH)

    def wo_block(cc, xx, zz, yy):
        row = ((cc * X + xx) * Z + zz) * PR
        return WO.at[:, pl.ds(pl.multiple_of(row, PR), PR), wo_columns(yy)]

    def wo_bundle(cc, xx, yy):
        row = (cc * X + xx) * Z * PR
        return WO.at[:, pl.ds(pl.multiple_of(row, PR), Z * PR), wo_columns(yy)]

    own_wo = wo_ref[...].astype(jnp.float32)
    for h in range(2):
        cols = [own_wo[:, i * HALF : (i + 1) * HALF] for i in range(h, 2 * X, 2)]
        WO_OWN[h] = jnp.concatenate(cols, axis=1).astype(jnp.bfloat16)
    wo_block(c, x, z, y)[...] = WO_OWN[...]
    pl.semaphore_wait(barrier, len(greeted))

    def w_unit(d, xx, cc, lanes):
        return W.at[zrel(d), w_rows(xx, cc), lanes[0] : lanes[1]]

    def w_bundle(xx, cc, lanes):
        return W.at[:, w_rows(xx, cc), lanes[0] : lanes[1]]

    def halves(lanes):
        middle = lanes[0] + -(-(lanes[1] - lanes[0]) // (2 * LANES)) * LANES
        return (lanes[0], middle), (middle, lanes[1])

    def along_x(d, lanes):
        for dx in x_near:
            unit = w_unit(d, x, c, lanes)
            links.send(("x1", lanes, d, dx), unit, unit, dev(dx=dx))

    def z_stage(lanes):
        for d in near_first:
            if d != 0:
                links.recv(("wz", lanes, d), w_unit(-d, x, c, lanes), dev(dz=-d))
            along_x(-d % Z, lanes)
        own = w_bundle(x, c, lanes)
        links.send(("wc", lanes, 0), own, own, dev(dc=1))

    def x_stage(lanes):
        for d in near_first:
            for dx, part in zip(x_near, halves(lanes)):
                links.recv(("x1", lanes, -d % Z, dx), w_unit(-d, xrel(-dx), c, lanes), dev(dx=-dx))
                if X > 2:
                    unit = w_unit(-d, xrel(-dx), c, part)
                    links.send(("x2", lanes, -d % Z, dx), unit, unit, dev(dx=dx))
        for dx in x_near:
            theirs = w_bundle(xrel(-dx), c, lanes)
            links.send(("wc", lanes, dx % X), theirs, theirs, dev(dc=1))

    def x_last(lanes):
        if X > 2:
            for d in near_first:
                for dx, part in zip(x_near, halves(lanes)):
                    unit = w_unit(-d, xrel(2), c, part)
                    links.recv(("x2", lanes, -d % Z, dx), unit, dev(dx=-dx))
                unit = w_unit(-d, xrel(2), c, lanes)
                links.send(("wc2", lanes, d), unit, unit, dev(dc=1))

    def core_last(lanes):
        for dx in [0] + [dx % X for dx in x_near]:
            links.recv(("wc", lanes, dx), w_bundle(xrel(-dx), co, lanes), dev(dc=1))
        if X > 2:
            for d in near_first:
                links.recv(("wc2", lanes, d), w_unit(-d, xrel(2), co, lanes), dev(dc=1))

    for lanes in (KVF, Q):
        for d in far_first:
            unit = w_unit(0, x, c, lanes)
            links.send(("wz", lanes, d), unit, unit, dev(dz=d))
    for dy in y_near:
        links.send(("tok", dy), t_rows(y), t_rows(y), dev(dy=dy))
    for d in far_first:
        links.send(("woz", d), WO_OWN, wo_block(c, x, z, y), dev(dz=d))

    QB[...] = jnp.zeros_like(QB)
    VT[:, HEAD_DIM:, :] = jnp.ones((2, VT.shape[1] - HEAD_DIM, VT.shape[2]), jnp.bfloat16)
    M[...] = jnp.full(M.shape, LOW, jnp.float32)
    ACC[...] = jnp.zeros_like(ACC)

    z_stage(KVF)
    for dy, lo in zip(y_near, (0, TB // 2)):
        links.recv(("tok", dy), t_rows(yrel(-dy)), dev(dy=-dy))
        if Y > 2:
            part = t_rows(yrel(-dy), lo, TB // 2)
            links.send(("tok2", dy), part, part, dev(dy=dy))
    x_stage(KVF)
    z_stage(Q)
    x_last(KVF)
    x_stage(Q)
    if Y > 2:
        for dy, lo in zip(y_near, (0, TB // 2)):
            links.recv(("tok2", dy), t_rows(yrel(2), lo, TB // 2), dev(dy=-dy))
    core_last(KVF)

    rows = XN[...]

    def project(lo, count):
        weight = W[:, :, lo : lo + count].reshape(D, count)
        return jnp.dot(rows, weight, preferred_element_type=jnp.float32)

    def slot(cc, zz, xx):
        return ((cc * Z + zz) * X + xx) * HB

    def k_block(cc, zz, xx):
        return K.at[pl.ds(pl.multiple_of(slot(cc, zz, xx), LANES), HB), :]

    def v_block(cc, zz, xx):
        return VT.at[:, 0:HEAD_DIM, pl.ds(pl.multiple_of(slot(cc, zz, xx), LANES), HB)]

    gates = project(2 * WC, LANES).T[:8]
    head_row = lax.broadcasted_iota(jnp.int32, gates.shape, 0)
    offset = jnp.zeros_like(gates)
    for h in range(X):
        offset = jnp.where(head_row == h, off_ref[h], offset)
    GS[...] = log_sigmoid(gates + offset + math.log(GB * Z * X * C))
    for dx in range(1, X):
        links.send(("g", dx), GS, GX.at[x], dev(dx=dx))
    GX[x] = GS[...]
    k_all = project(0, WC)
    for h in range(X):
        kh = k_all[:, h * HEAD_DIM : (h + 1) * HEAD_DIM]
        KS[h] = jnp.concatenate([kh[:HB], kh[HB:]], axis=1).astype(jnp.bfloat16)
    for dx in range(1, X):
        links.send(("k", dx), KS.at[xrel(dx)], k_block(c, z, x), dev(dx=dx))
    x_last(Q)
    v_all = project(WC, WC).T
    for h in range(X):
        vh = v_all[h * HEAD_DIM : (h + 1) * HEAD_DIM].astype(jnp.bfloat16)
        VS[h, 0] = vh[:, :HB]
        VS[h, 1] = vh[:, HB:]
    for dx in range(1, X):
        links.send(("v", dx), VS.at[xrel(dx)], v_block(c, z, x), dev(dx=dx))
    k_block(c, z, x)[...] = KS[x]
    v_block(c, z, x)[...] = VS[x]

    UP = DN = Z // 2

    def goes(way, a, k):
        return k < UP or (k == UP and (a == 0) == (way == "up"))

    def bundle(zz, cc):
        at = pl.multiple_of(slot(cc, zz, 0), LANES)
        return K.at[pl.ds(at, X * HB), :], VT.at[:, 0:HEAD_DIM, pl.ds(at, X * HB)]

    def piece(zz, dx):
        return k_block(c, zz, xrel(-dx)), v_block(c, zz, xrel(-dx))

    WAYS = (("up", 1), ("dn", -1))
    pieces = [0] + ([1, X - 1] if X > 2 else [1]) + list(range(2, X - 1))

    def ring_start(dx):
        for a, view in enumerate(piece(z, dx)):
            for way, sign in WAYS:
                if goes(way, a, 1):
                    links.send((way, 1, dx, a), view, view, dev(dz=sign))

    def to_core(d):
        for a, view in enumerate(bundle(zrel(d), c)):
            links.send(("core", d % Z, a), view, view, dev(dc=1))

    def ring_step(k, some):
        for dx in some:
            for a in range(2):
                for way, sign in WAYS:
                    if goes(way, a, k):
                        view = piece(zrel(-sign * k), dx)[a]
                        links.recv((way, k, dx, a), view, dev(dz=-sign))
                        if goes(way, a, k + 1):
                            links.send((way, k + 1, dx, a), view, view, dev(dz=sign))

    def other_core(d):
        for a, view in enumerate(bundle(zrel(d), co)):
            links.recv(("core", d % Z, a), view, dev(dc=1))

    ring_start(0)
    core_last(Q)
    q_all = project(KVF[1], WC)
    q_all = q_all.astype(jnp.bfloat16).astype(jnp.float32) * (HEAD_DIM**-0.5 * LOG2E)
    q_all = q_all.T
    for h in range(X):
        QS[h] = q_all[h * HEAD_DIM : (h + 1) * HEAD_DIM].astype(jnp.bfloat16)
    for dx in range(1, X):
        links.send(("q", dx), QS.at[xrel(dx)], QT.at[x], dev(dx=dx))
    QT[x] = QS[x]

    for dx in range(1, X):
        links.recv(("g", dx), GX.at[xrel(-dx)], dev(dx=-dx))
    row8 = lax.broadcasted_iota(jnp.int32, (8, GB), 0)
    own_gates = jnp.zeros((8, GB), jnp.float32)
    for sx in range(X):
        picked = jnp.sum(jnp.where(row8 == x, GX[sx], 0.0), axis=0, keepdims=True)
        own_gates = jnp.where(row8 == sx, picked, own_gates)
    GP[...] = own_gates
    links.send(("gp",), GP, GPR, dev(dc=1))
    links.recv(("gp",), GPR, dev(dc=1))
    theirs = GPR[...]
    chip_gates = jnp.zeros((8, GB), jnp.float32)
    for sx in range(X):
        a, b = own_gates[sx : sx + 1], theirs[sx : sx + 1]
        chip_gates = jnp.where(row8 == 2 * sx, jnp.where(c == 0, a, b), chip_gates)
        chip_gates = jnp.where(row8 == 2 * sx + 1, jnp.where(c == 0, b, a), chip_gates)
    G[z] = chip_gates
    for d in far_first:
        links.send(("gz", d), G.at[z], G.at[z], dev(dz=d))
    for dx in pieces[1:]:
        sx = xrel(-dx)
        links.recv(("k", dx), k_block(c, z, sx), dev(dx=-dx))
        links.recv(("v", dx), v_block(c, z, sx), dev(dx=-dx))
        ring_start(dx)
    to_core(0)

    for dx in range(1, X):
        links.recv(("q", dx), QT.at[xrel(-dx)], dev(dx=-dx))
    for sx in range(X):
        QB[sx, 0:HEAD_DIM, 0:GB] = QT[sx]
        QB[sx, HEAD_DIM:, GB:] = QT[sx]
    for d in far_first:
        links.recv(("woz", d), wo_block(c, x, zrel(-d), y), dev(dz=-d))
    own = wo_bundle(c, x, y)
    for dx, dy in plane:
        links.send(("woxy", dx, dy), own, own, dev(dx=dx, dy=dy))
    links.send(("woc", 0, 0), own, own, dev(dc=1))

    def cumulative(block):
        n = block.shape[0]
        lane = lax.broadcasted_iota(jnp.int32, block.shape, 1)
        step = 1
        while step < GB:
            block = block + jnp.where(lane >= step, pltpu.roll(block, step, 1), 0.0)
            step *= 2
        total = jnp.broadcast_to(block[:, GB - 1 :], (n, LANES))
        row = lax.broadcasted_iota(jnp.int32, total.shape, 0)
        before = jnp.where(row >= 1, pltpu.roll(total, 1, 0), 0.0)
        step = 1
        while step < n:
            before = before + jnp.where(row >= step, pltpu.roll(before, step, 0), 0.0)
            step *= 2
        return (block + before[:, 0:1]) * LOG2E

    def query_sums(block):
        return [
            jnp.sum(jnp.where(row8 == 2 * sx + c, block, 0.0), axis=0, keepdims=True)
            for sx in range(X)
        ]

    def key_sums(block, cc):
        block = jnp.where(cc == 0, block, pltpu.roll(block, 7, 0))
        both = jnp.concatenate([block[:, :HB], block[:, HB:]], axis=0)
        both = jnp.concatenate([both, jnp.zeros((LANES - 16, HB), jnp.float32)], axis=0)
        return both.T

    def attend(items, cum_q):
        AHEAD, SOFT = 3, 1
        n_s, n_p = AHEAD - SOFT + 1, SOFT + 1
        best, rescale, loaded = {}, {}, {}

        def prepared(table, at, pair):
            key = (id(table), pair)
            if key not in loaded:
                even, odd = 4 * pair, 4 * pair + 2
                b0 = [table[:, even : even + 1], table[:, odd : odd + 1]]
                b1 = [table[:, 8 + even : 9 + even], table[:, 8 + odd : 9 + odd]]
                start = pl.multiple_of(at + pair * 2 * HB, 2 * HB)
                loaded[key] = jnp.concatenate(b0, axis=0), jnp.concatenate(b1, axis=0), start
            return loaded[key]

        def scores(j):
            table, at, pair, t, mask = items[j]
            b0, b1, start = prepared(table, at, pair)
            s = jnp.dot(K[pl.ds(start, 2 * HB), :], QB[t], preferred_element_type=jnp.float32)
            s0, s1 = s[:, :GB] - b0, s[:, GB:] - b1
            if mask is not None:
                s0, s1 = mask(s0, 0, t), mask(s1, 1, t)
            SC[j % n_s, 0], SC[j % n_s, 1] = s0, s1
            best[j] = jnp.maximum(jnp.max(s0, axis=0, keepdims=True), jnp.max(s1, axis=0, keepdims=True))

        def softmax(j):
            t = items[j][3]
            old = M[t]
            new = jnp.maximum(old, best[j] + cum_q[t])
            rescale[j] = jnp.exp2(old - new)
            M[t] = new
            shift = new - cum_q[t]
            PB[j % n_p, : 2 * HB] = jnp.exp2(SC[j % n_s, 0] - shift).astype(jnp.bfloat16)
            PB[j % n_p, 2 * HB :] = jnp.exp2(SC[j % n_s, 1] - shift).astype(jnp.bfloat16)

        def weigh(j):
            table, at, pair, t, _ = items[j]
            start = prepared(table, at, pair)[2]
            v = jnp.concatenate(
                [VT[0, :, pl.ds(start, 2 * HB)], VT[1, :, pl.ds(start, 2 * HB)]], axis=1
            )
            ACC[t] = ACC[t] * rescale[j] + jnp.dot(
                v, PB[j % n_p], preferred_element_type=jnp.float32
            )

        for j in range(-AHEAD, len(items)):
            if 0 <= j + AHEAD < len(items):
                scores(j + AHEAD)
            if j >= 0:
                weigh(j)
            if 0 <= j + SOFT < len(items):
                softmax(j + SOFT)

    cum_here = cumulative(G[z])
    cum_q_here = query_sums(cum_here)

    def present(cc):
        def masked(pair):
            def mask(s, which, t):
                r = lax.broadcasted_iota(jnp.int32, s.shape, 0)
                first = 4 * pair + cc
                key = jnp.where(r < HB, first * GB + r, (first + 2) * GB + r - HB) + which * HB
                query = (2 * t + c) * GB + lax.broadcasted_iota(jnp.int32, s.shape, 1)
                return jnp.where(key <= query, s, LOW)

            return mask

        table = key_sums(cum_here, cc)
        items = [
            (table, slot(cc, z, 0), pair, t, masked(pair) if t <= 2 * pair + 1 else None)
            for pair in range(X // 2)
            for t in range(2 * pair, X)
        ]
        attend(items, cum_q_here)

    def past(ds, cc):
        items = []
        for d in ds:
            zz = zrel(d)
            table = key_sums(CUM[zz], cc)
            items += [
                (table, slot(cc, zz, 0), pair, t, None) for pair in range(X // 2) for t in range(X)
            ]
        attend(items, query_sums(CUM[z]))

    def wo_forward():
        for dx, dy in plane:
            theirs = wo_bundle(c, xrel(-dx), yrel(-dy))
            links.recv(("woxy", dx, dy), theirs, dev(dx=-dx, dy=-dy))
            links.send(("woc", dx, dy), theirs, theirs, dev(dc=1))

    def step_back(k, cc):
        if k == 0:
            present(cc)
        elif k < UP:

            @pl.when(z + k >= Z)
            def _():
                past([-k, k], cc)

            @pl.when((z >= k) & (z + k < Z))
            def _():
                past([-k], cc)

        else:

            @pl.when(z >= k)
            def _():
                past([-k], cc)

    def came(k):
        for d in [-k, k] if 0 < k < UP else [-k]:
            other_core(d)

    cut = (len(pieces) + 1) // 2
    for k in range(1, UP + 1):
        ring_step(k, pieces[:cut])
        step_back(k - 1, c)
        ring_step(k, pieces[cut:])
        to_core(-k)
        if k < UP:
            to_core(k)
        if k == UP:
            wo_forward()
        came(k - 1)
        step_back(k - 1, co)
        if k == 1:
            for d in far_first:
                links.recv(("gz", d), G.at[zrel(-d)], dev(dz=-d))
            CUM[...] = cumulative(G[...].reshape(Z * 8, GB)).reshape(Z, 8, GB)
    step_back(UP, c)
    came(UP)
    step_back(UP, co)

    for t in range(X):
        acc = ACC[t]
        o = (acc[:HEAD_DIM] / acc[HEAD_DIM : HEAD_DIM + 1]).astype(jnp.bfloat16)
        for yy in range(Y):
            part = o[:, yy * TB : (yy + 1) * TB]
            for h in range(2):
                OS[t, yy, :, h * TB : (h + 1) * TB] = part[h * HALF : (h + 1) * HALF]

    def at_rows(xx, yy):
        return AT.at[pl.ds(pl.multiple_of((yy * X + xx) * HALF, HALF), HALF), :]

    for dx, dy in plane:
        links.send(("o", dx, dy), OS.at[xrel(dx), yrel(dy)], at_rows(x, y), dev(dx=dx, dy=dy))
    at_rows(x, y)[...] = OS[x, y]
    for dx in range(X):
        for dy in range(Y):
            theirs = wo_bundle(co, xrel(-dx), yrel(-dy))
            links.recv(("woc", dx, dy), theirs, dev(dc=1))
    for dx, dy in plane:
        links.recv(("o", dx, dy), at_rows(xrel(-dx), yrel(-dy)), dev(dx=-dx, dy=-dy))

    attended = AT[...]
    for cc in range(C):
        for xx in range(X):
            block = (cc * X + xx) * Z * PR
            part = sum(
                jnp.dot(WO[h, block : block + Z * PR, :], attended, preferred_element_type=jnp.float32)[
                    :, h * TB : (h + 1) * TB
                ]
                for h in range(2)
            )
            for zz in range(Z):
                to = ((zz * X + xx) * C + cc) * PR
                PT[to : to + PR, 0:TB] = part[zz * PR : (zz + 1) * PR]
    out_ref[...] = rms_norm(PT[...].T[:TB], ogain_ref[...])
    links.drain()


def layer(dims, tokens, norm_gain, w_query, w_key, w_value, w_forget, forget_offset, w_out_t, out_gain):
    Z, X, C, Y = dims
    TB, D = tokens.shape
    PR, WC = w_query.shape
    GB = TB * Y
    HB = GB // 2
    LW = 3 * WC + LANES
    keys = Z * X * C * HB
    n_sems = 340
    vmem, smem = pl.BlockSpec(memory_space=pltpu.VMEM), pl.BlockSpec(memory_space=pltpu.SMEM)
    bf16, f32 = jnp.bfloat16, jnp.float32
    scratch = [
        pltpu.VMEM((Z, X * C * PR, LW), bf16),
        pltpu.VMEM((GB, D), bf16),
        pltpu.VMEM((2, D, D // 2), bf16),
        pltpu.VMEM((X, HB, LANES), bf16),
        pltpu.VMEM((X, 2, HEAD_DIM, HB), bf16),
        pltpu.VMEM((X, HEAD_DIM, GB), bf16),
        pltpu.VMEM((8, GB), f32),
        pltpu.VMEM((X, 8, GB), f32),
        pltpu.VMEM((8, GB), f32),
        pltpu.VMEM((8, GB), f32),
        pltpu.VMEM((Z, 8, GB), f32),
        pltpu.VMEM((Z, 8, GB), f32),
        pltpu.VMEM((keys, LANES), bf16),
        pltpu.VMEM((2, HEAD_DIM + 16, keys), bf16),
        pltpu.VMEM((X, HEAD_DIM, GB), bf16),
        pltpu.VMEM((X, LANES, 2 * GB), bf16),
        pltpu.VMEM((X, 1, GB), f32),
        pltpu.VMEM((X, HEAD_DIM + 16, GB), f32),
        pltpu.VMEM((X, Y, HEAD_DIM // 2, 2 * TB), bf16),
        pltpu.VMEM((D // 2, 2 * TB), bf16),
        pltpu.VMEM((D, LANES), f32),
        pltpu.VMEM((3, 2, 2 * HB, GB), f32),
        pltpu.VMEM((2, 4 * HB, GB), bf16),
        pltpu.VMEM((2, PR, WC // 2), bf16),
        pltpu.SemaphoreType.DMA((n_sems,)),
        pltpu.SemaphoreType.DMA((n_sems,)),
    ]
    return pl.pallas_call(
        functools.partial(kernel, dims),
        out_shape=jax.ShapeDtypeStruct((TB, D), bf16),
        in_specs=[vmem] * 6 + [smem, vmem, vmem],
        out_specs=vmem,
        scratch_shapes=scratch,
        compiler_params=pltpu.CompilerParams(
            collective_id=0, has_side_effects=True, vmem_limit_bytes=56 * 1024 * 1024
        ),
    )(
        tokens,
        norm_gain.reshape(1, D),
        w_query,
        w_key,
        w_value,
        w_forget.T,
        forget_offset,
        w_out_t,
        out_gain.reshape(1, D),
    )


def sharded(mesh, dims):
    finer = Mesh(mesh.devices.reshape(*dims), AXES)
    sp = ("z", "x", "c")
    return jax.shard_map(
        functools.partial(layer, dims),
        mesh=finer,
        in_specs=(
            P(AXES, None),
            P(),
            P(sp, "y"),
            P(sp, "y"),
            P(sp, "y"),
            P(sp, "y"),
            P("y"),
            P(sp, "y"),
            P(),
        ),
        out_specs=P(AXES, None),
        check_vma=False,
    )


def solution(mesh):
    return sharded(mesh, (8, 4, 2, mesh.shape["tp"]))
```

```python
import functools
import math

import jax
import jax.numpy as jnp
from jax import lax
from jax.experimental import pallas as pl
from jax.experimental.pallas import tpu as pltpu
from jax.sharding import Mesh
from jax.sharding import PartitionSpec as P

HEAD_DIM = 64
AXES = ("z", "x", "c", "y")
MESH = pl.DeviceIdType.MESH
EPS = 1e-06
LOG2E = 1.4426950408889634
LOW = -1e30
LANES = 128


def rms_norm(floats, gain_row):
    scale_row = lax.rsqrt(jnp.mean(floats * floats, axis=-1, keepdims=True) + EPS)
    return (floats * scale_row * gain_row).astype(jnp.bfloat16)


def log_sigmoid(t):
    u = jnp.exp(-jnp.abs(t))
    series = u * (1.0 - u * (0.5 - u * (1.0 / 3.0 - u * 0.25)))
    return jnp.minimum(t, 0.0) - jnp.where(u < 0.01, series, jnp.log(1.0 + u))


class Links:
    def __init__(self, send_sems, recv_sems, counter):
        self.send_sems, self.recv_sems, self.counter = send_sems, recv_sems, counter
        self.ids, self.sent = {}, [0]
        self.most = counter.shape[0]

    def copy(self, key, src, dst, dev):
        return pltpu.make_async_remote_copy(
            src_ref=src,
            dst_ref=dst,
            send_sem=self.send_sems.at[len(self.sent) - 1],
            recv_sem=self.recv_sems.at[self.ids.setdefault(key, len(self.ids))],
            device_id=dev,
            device_id_type=MESH,
        )

    def send(self, key, src, dst, dev):
        rows = math.prod(src.shape) * src.dtype.itemsize // (2 * LANES)
        if self.sent[-1] + rows > self.most:
            self.sent.append(0)
        self.sent[-1] += rows
        self.copy(key, src, dst, dev).start()

    def recv(self, key, landed, dev):
        self.copy(key, landed, landed, dev).wait_recv()

    def drain(self, dev):
        for at, rows in enumerate(self.sent):
            view = self.counter.at[0:rows]
            pltpu.make_async_remote_copy(
                src_ref=view,
                dst_ref=view,
                send_sem=self.send_sems.at[at],
                recv_sem=self.recv_sems.at[0],
                device_id=dev,
                device_id_type=MESH,
            ).wait_send()


def kernel(
    dims,
    tokens_ref,
    gain_ref,
    wq_ref,
    wk_ref,
    wv_ref,
    wf_ref,
    off_ref,
    wo_ref,
    ogain_ref,
    out_ref,
    W,
    XN,
    WO,
    KS,
    VS,
    QS,
    GS,
    GX,
    GP,
    GPR,
    G,
    CUM,
    K,
    VT,
    QT,
    QB,
    M,
    ACC,
    OS,
    AT,
    PT,
    SC,
    PB,
    WO_OWN,
    send_sems,
    recv_sems,
):
    Z, X, C, Y = dims
    TB, D = tokens_ref.shape
    GB = TB * Y
    HB = GB // 2
    PR, WC = wo_ref.shape
    LW = W.shape[2]
    z, x, c, y = (lax.axis_index(a) for a in AXES)
    links = Links(send_sems, recv_sems, K)

    def dev(dz=0, dx=0, dc=0, dy=0):
        return {
            "z": lax.rem(z + (dz % Z), Z),
            "x": lax.rem(x + (dx % X), X),
            "c": lax.rem(c + (dc % C), C),
            "y": lax.rem(y + (dy % Y), Y),
        }

    def zrel(d):
        return lax.rem(z + (d % Z), Z)

    def xrel(d):
        return lax.rem(x + (d % X), X)

    def yrel(d):
        return lax.rem(y + (d % Y), Y)

    co = 1 - c
    plane = [(dx, dy) for dx in range(X) for dy in range(Y) if (dx, dy) != (0, 0)]
    far_first = sorted(range(1, Z), key=lambda d: -min(d, Z - d))
    near_first = [0] + far_first[::-1]
    x_near, y_near = ([1] if n == 2 else [1, -1] for n in (X, Y))

    barrier = pltpu.get_barrier_semaphore()
    greeted = (
        [dict(dx=dx, dy=dy) for dx, dy in plane] + [dict(dc=1)] + [dict(dz=d) for d in range(1, Z)]
    )
    for g in greeted:
        pl.semaphore_signal(barrier, inc=1, device_id=dev(**g), device_id_type=MESH)

    def w_rows(xx, cc):
        return pl.ds(pl.multiple_of((xx * C + cc) * PR, PR), PR)

    KVF, Q = (0, 2 * WC + LANES), (2 * WC + LANES, LW)
    mine = w_rows(x, c)
    W[z, mine, 0:WC] = wk_ref[...]
    W[z, mine, WC : 2 * WC] = wv_ref[...]
    W[z, mine, KVF[1] :] = wq_ref[...]
    PT[0:LANES] = jnp.zeros((LANES, LANES), jnp.float32)
    PT[0:X, 0:PR] = wf_ref[...].astype(jnp.float32)
    W[z, mine, 2 * WC : KVF[1]] = PT[0:LANES].T[:PR].astype(jnp.bfloat16)

    def t_rows(yy, lo=0, count=TB):
        return XN.at[pl.ds(pl.multiple_of(yy * TB + lo, 32), count), :]

    t_rows(y)[...] = rms_norm(tokens_ref[...].astype(jnp.float32), gain_ref[...])

    HALF = HEAD_DIM // 2
    WH = WC // 2

    def wo_columns(yy):
        return pl.ds(pl.multiple_of(yy * WH, WH), WH)

    def wo_block(cc, xx, zz, yy):
        row = ((cc * X + xx) * Z + zz) * PR
        return WO.at[:, pl.ds(pl.multiple_of(row, PR), PR), wo_columns(yy)]

    def wo_bundle(cc, xx, yy):
        row = (cc * X + xx) * Z * PR
        return WO.at[:, pl.ds(pl.multiple_of(row, PR), Z * PR), wo_columns(yy)]

    own_wo = wo_ref[...].astype(jnp.float32)
    for h in range(2):
        cols = [own_wo[:, i * HALF : (i + 1) * HALF] for i in range(h, 2 * X, 2)]
        WO_OWN[h] = jnp.concatenate(cols, axis=1).astype(jnp.bfloat16)
    wo_block(c, x, z, y)[...] = WO_OWN[...]
    pl.semaphore_wait(barrier, len(greeted))

    def w_unit(d, xx, cc, lanes):
        return W.at[zrel(d), w_rows(xx, cc), lanes[0] : lanes[1]]

    def w_bundle(xx, cc, lanes):
        return W.at[:, w_rows(xx, cc), lanes[0] : lanes[1]]

    def halves(lanes):
        middle = lanes[0] + -(-(lanes[1] - lanes[0]) // (2 * LANES)) * LANES
        return (lanes[0], middle), (middle, lanes[1])

    opposite = X > 2

    def fine_z(i, d):
        if d != 0:
            links.recv(("wz", d), w_unit(-d, x, c, KVF), dev(dz=-d))
        for dx in x_near:
            unit = w_unit(-d, x, c, KVF)
            links.send(("x1", d, dx), unit, unit, dev(dx=dx))

    def fine_x(d):
        for dx, part in zip(x_near, halves(KVF)):
            links.recv(("x1", d, dx), w_unit(-d, xrel(-dx), c, KVF), dev(dx=-dx))
            if opposite:
                unit = w_unit(-d, xrel(-dx), c, part)
                links.send(("x2", d, dx), unit, unit, dev(dx=dx))

    def fine_last(d):
        for dx, part in zip(x_near, halves(KVF)):
            links.recv(("x2", d, dx), w_unit(-d, xrel(2), c, part), dev(dx=-dx))
        unit = w_unit(-d, xrel(2), c, KVF)
        links.send(("wc", KVF), unit, unit, dev(dc=1))

    def to_other_core(xx, lanes):
        view = w_bundle(xx, c, lanes)
        links.send(("wc", lanes), view, view, dev(dc=1))

    def core_last(lanes):
        links.recv(("wc", lanes), W.at[:, 0 : X * PR, lanes[0] : lanes[1]], dev(dc=1))

    for lanes in (KVF, Q):
        for d in far_first:
            unit = w_unit(0, x, c, lanes)
            links.send(("wz", d if lanes == KVF else Q), unit, unit, dev(dz=d))
    for dy in y_near:
        links.send(("tok", dy), t_rows(y), t_rows(y), dev(dy=dy))
    for d in far_first:
        links.send(("woz",), WO_OWN, wo_block(c, x, z, y), dev(dz=d))

    QB[...] = jnp.zeros_like(QB)
    VT[:, HEAD_DIM:, :] = jnp.ones((2, VT.shape[1] - HEAD_DIM, VT.shape[2]), jnp.bfloat16)
    M[...] = jnp.full(M.shape, LOW, jnp.float32)
    ACC[...] = jnp.zeros_like(ACC)

    LAG = 3
    for i in range(Z + LAG):
        if i < Z:
            fine_z(i, near_first[i])
        if i >= LAG:
            fine_x(near_first[i - LAG])
        if i == min(5, Z):
            for dy, lo in zip(y_near, (0, TB // 2)):
                links.recv(("tok", dy), t_rows(yrel(-dy)), dev(dy=-dy))
                if Y > 2:
                    part = t_rows(yrel(-dy), lo, TB // 2)
                    links.send(("tok2", dy), part, part, dev(dy=dy))
    for dx in [0] + x_near:
        to_other_core(xrel(-dx), KVF)
    links.recv(("wz", Q), W.at[0 : Z - 1, 0:PR, Q[0] : Q[1]], dev(dz=1))
    for dx in x_near:
        view = w_bundle(x, c, Q)
        links.send(("x1", Q, dx), view, view, dev(dx=dx))
    if opposite:
        for d in near_first:
            fine_last(d)
    for dx, part in zip(x_near, halves(Q)):
        links.recv(("x1", Q, dx), w_bundle(xrel(-dx), c, Q), dev(dx=-dx))
        if opposite:
            view = w_bundle(xrel(-dx), c, part)
            links.send(("x2", Q, dx), view, view, dev(dx=dx))
    for dx in [0] + x_near:
        to_other_core(xrel(-dx), Q)
    if Y > 2:
        for dy, lo in zip(y_near, (0, TB // 2)):
            links.recv(("tok2", dy), t_rows(yrel(2), lo, TB // 2), dev(dy=-dy))
    core_last(KVF)

    rows = XN[...]

    def project(lo, count):
        weight = W[:, :, lo : lo + count].reshape(D, count)
        return jnp.dot(rows, weight, preferred_element_type=jnp.float32)

    def slot(cc, zz, xx):
        return ((cc * Z + zz) * X + xx) * HB

    def k_block(cc, zz, xx):
        return K.at[pl.ds(pl.multiple_of(slot(cc, zz, xx), LANES), HB), :]

    def v_block(cc, zz, xx):
        return VT.at[:, 0:HEAD_DIM, pl.ds(pl.multiple_of(slot(cc, zz, xx), LANES), HB)]

    gates = project(2 * WC, LANES).T[:8]
    head_row = lax.broadcasted_iota(jnp.int32, gates.shape, 0)
    offset = jnp.zeros_like(gates)
    for h in range(X):
        offset = jnp.where(head_row == h, off_ref[h], offset)
    GS[...] = log_sigmoid(gates + offset + math.log(GB * Z * X * C))
    for dx in range(1, X):
        links.send(("g",), GS, GX.at[x], dev(dx=dx))
    GX[x] = GS[...]
    k_all = project(0, WC)
    for h in range(X):
        kh = k_all[:, h * HEAD_DIM : (h + 1) * HEAD_DIM]
        KS[h] = jnp.concatenate([kh[:HB], kh[HB:]], axis=1).astype(jnp.bfloat16)
    for dx in range(1, X):
        links.send(("kv", dx), KS.at[xrel(dx)], k_block(c, z, x), dev(dx=dx))
    if opposite:
        for dx, part in zip(x_near, halves(Q)):
            links.recv(("x2", Q, dx), w_bundle(xrel(2), c, part), dev(dx=-dx))
        to_other_core(xrel(2), Q)
    v_all = project(WC, WC).T
    for h in range(X):
        vh = v_all[h * HEAD_DIM : (h + 1) * HEAD_DIM].astype(jnp.bfloat16)
        VS[h, 0] = vh[:, :HB]
        VS[h, 1] = vh[:, HB:]
    for dx in range(1, X):
        links.send(("kv", dx), VS.at[xrel(dx)], v_block(c, z, x), dev(dx=dx))
    k_block(c, z, x)[...] = KS[x]
    v_block(c, z, x)[...] = VS[x]

    UP = DN = Z // 2

    def goes(way, a, k):
        return k < UP or (k == UP and (a == 0) == (way == "up"))

    def bundle(zz, cc):
        at = pl.multiple_of(slot(cc, zz, 0), LANES)
        return K.at[pl.ds(at, X * HB), :], VT.at[:, 0:HEAD_DIM, pl.ds(at, X * HB)]

    def piece(zz, dx):
        return k_block(c, zz, xrel(-dx)), v_block(c, zz, xrel(-dx))

    WAYS = (("up", 1), ("dn", -1))
    pieces = [0] + ([1, X - 1] if X > 2 else [1]) + list(range(2, X - 1))

    def ring_start(dx):
        for a, view in enumerate(piece(z, dx)):
            for way, sign in WAYS:
                if goes(way, a, 1):
                    links.send((way, 1, dx), view, view, dev(dz=sign))

    def to_core(d):
        for view in bundle(zrel(d), c):
            links.send(("core", d % Z), view, view, dev(dc=1))

    def ring_step(k, some):
        for dx in some:
            for way, sign in WAYS:
                arrays = [a for a in range(2) if goes(way, a, k)]
                links.recv((way, k, dx), K.at[0 : len(arrays) * HB], dev(dz=-sign))
                for a in arrays:
                    if goes(way, a, k + 1):
                        view = piece(zrel(-sign * k), dx)[a]
                        links.send((way, k + 1, dx), view, view, dev(dz=sign))

    def other_core(d):
        links.recv(("core", d % Z), K.at[0 : 2 * X * HB], dev(dc=1))

    ring_start(0)
    core_last(Q)
    q_all = project(KVF[1], WC)
    q_all = q_all.astype(jnp.bfloat16).astype(jnp.float32) * (HEAD_DIM**-0.5 * LOG2E)
    q_all = q_all.T
    for h in range(X):
        QS[h] = q_all[h * HEAD_DIM : (h + 1) * HEAD_DIM].astype(jnp.bfloat16)
    for dx in range(1, X):
        links.send(("q",), QS.at[xrel(dx)], QT.at[x], dev(dx=dx))
    QT[x] = QS[x]

    links.recv(("g",), GX.at[0 : X - 1], dev(dx=1))
    row8 = lax.broadcasted_iota(jnp.int32, (8, GB), 0)
    own_gates = jnp.zeros((8, GB), jnp.float32)
    for sx in range(X):
        picked = jnp.sum(jnp.where(row8 == x, GX[sx], 0.0), axis=0, keepdims=True)
        own_gates = jnp.where(row8 == sx, picked, own_gates)
    GP[...] = own_gates
    links.send(("gp",), GP, GPR, dev(dc=1))
    links.recv(("gp",), GPR, dev(dc=1))
    theirs = GPR[...]
    chip_gates = jnp.zeros((8, GB), jnp.float32)
    for sx in range(X):
        a, b = own_gates[sx : sx + 1], theirs[sx : sx + 1]
        chip_gates = jnp.where(row8 == 2 * sx, jnp.where(c == 0, a, b), chip_gates)
        chip_gates = jnp.where(row8 == 2 * sx + 1, jnp.where(c == 0, b, a), chip_gates)
    G[z] = chip_gates
    for d in far_first:
        links.send(("gz",), G.at[z], G.at[z], dev(dz=d))
    for dx in pieces[1:]:
        links.recv(("kv", dx), K.at[0 : 2 * HB], dev(dx=-dx))
        ring_start(dx)
    to_core(0)

    links.recv(("q",), QT.at[0 : X - 1], dev(dx=1))
    for sx in range(X):
        QB[sx, 0:HEAD_DIM, 0:GB] = QT[sx]
        QB[sx, HEAD_DIM:, GB:] = QT[sx]
    links.recv(("woz",), WO.at[:, 0 : (Z - 1) * PR, 0:WH], dev(dz=1))
    own = wo_bundle(c, x, y)
    for dx, dy in plane:
        links.send(("woxy",), own, own, dev(dx=dx, dy=dy))
    links.send(("woc",), own, own, dev(dc=1))

    def cumulative(block):
        n = block.shape[0]
        lane = lax.broadcasted_iota(jnp.int32, block.shape, 1)
        step = 1
        while step < GB:
            block = block + jnp.where(lane >= step, pltpu.roll(block, step, 1), 0.0)
            step *= 2
        total = jnp.broadcast_to(block[:, GB - 1 :], (n, LANES))
        row = lax.broadcasted_iota(jnp.int32, total.shape, 0)
        before = jnp.where(row >= 1, pltpu.roll(total, 1, 0), 0.0)
        step = 1
        while step < n:
            before = before + jnp.where(row >= step, pltpu.roll(before, step, 0), 0.0)
            step *= 2
        return (block + before[:, 0:1]) * LOG2E

    def query_sums(block):
        return [
            jnp.sum(jnp.where(row8 == 2 * sx + c, block, 0.0), axis=0, keepdims=True)
            for sx in range(X)
        ]

    def key_sums(block, cc):
        block = jnp.where(cc == 0, block, pltpu.roll(block, 7, 0))
        both = jnp.concatenate([block[:, :HB], block[:, HB:]], axis=0)
        both = jnp.concatenate([both, jnp.zeros((LANES - 16, HB), jnp.float32)], axis=0)
        return both.T

    def attend(items, cum_q):
        AHEAD, SOFT = 3, 1
        n_s, n_p = AHEAD - SOFT + 1, SOFT + 1
        best, rescale, loaded = {}, {}, {}

        def prepared(table, at, pair):
            key = (id(table), pair)
            if key not in loaded:
                even, odd = 4 * pair, 4 * pair + 2
                b0 = [table[:, even : even + 1], table[:, odd : odd + 1]]
                b1 = [table[:, 8 + even : 9 + even], table[:, 8 + odd : 9 + odd]]
                start = pl.multiple_of(at + pair * 2 * HB, 2 * HB)
                loaded[key] = jnp.concatenate(b0, axis=0), jnp.concatenate(b1, axis=0), start
            return loaded[key]

        def scores(j):
            table, at, pair, t, mask = items[j]
            b0, b1, start = prepared(table, at, pair)
            s = jnp.dot(K[pl.ds(start, 2 * HB), :], QB[t], preferred_element_type=jnp.float32)
            s0, s1 = s[:, :GB] - b0, s[:, GB:] - b1
            if mask is not None:
                s0, s1 = mask(s0, 0, t), mask(s1, 1, t)
            SC[j % n_s, 0], SC[j % n_s, 1] = s0, s1
            best[j] = jnp.maximum(jnp.max(s0, axis=0, keepdims=True), jnp.max(s1, axis=0, keepdims=True))

        def softmax(j):
            t = items[j][3]
            old = M[t]
            new = jnp.maximum(old, best[j] + cum_q[t])
            rescale[j] = jnp.exp2(old - new)
            M[t] = new
            shift = new - cum_q[t]
            PB[j % n_p, : 2 * HB] = jnp.exp2(SC[j % n_s, 0] - shift).astype(jnp.bfloat16)
            PB[j % n_p, 2 * HB :] = jnp.exp2(SC[j % n_s, 1] - shift).astype(jnp.bfloat16)

        def weigh(j):
            table, at, pair, t, _ = items[j]
            start = prepared(table, at, pair)[2]
            v = jnp.concatenate(
                [VT[0, :, pl.ds(start, 2 * HB)], VT[1, :, pl.ds(start, 2 * HB)]], axis=1
            )
            ACC[t] = ACC[t] * rescale[j] + jnp.dot(
                v, PB[j % n_p], preferred_element_type=jnp.float32
            )

        for j in range(-AHEAD, len(items)):
            if 0 <= j + AHEAD < len(items):
                scores(j + AHEAD)
            if j >= 0:
                weigh(j)
            if 0 <= j + SOFT < len(items):
                softmax(j + SOFT)

    cum_here = cumulative(G[z])
    cum_q_here = query_sums(cum_here)

    def present(cc):
        def masked(pair):
            def mask(s, which, t):
                r = lax.broadcasted_iota(jnp.int32, s.shape, 0)
                first = 4 * pair + cc
                key = jnp.where(r < HB, first * GB + r, (first + 2) * GB + r - HB) + which * HB
                query = (2 * t + c) * GB + lax.broadcasted_iota(jnp.int32, s.shape, 1)
                return jnp.where(key <= query, s, LOW)

            return mask

        table = key_sums(cum_here, cc)
        items = [
            (table, slot(cc, z, 0), pair, t, masked(pair) if t <= 2 * pair + 1 else None)
            for pair in range(X // 2)
            for t in range(2 * pair, X)
        ]
        attend(items, cum_q_here)

    def past(ds, cc):
        items = []
        for d in ds:
            zz = zrel(d)
            table = key_sums(CUM[zz], cc)
            items += [
                (table, slot(cc, zz, 0), pair, t, None) for pair in range(X // 2) for t in range(X)
            ]
        attend(items, query_sums(CUM[z]))

    def wo_rows(bundles):
        return bundles * Z * PR * WH // WO.shape[2]

    def wo_forward():
        links.recv(("woxy",), WO.at[:, 0 : wo_rows(len(plane)), :], dev(dx=1))
        for dx, dy in plane:
            theirs = wo_bundle(c, xrel(-dx), yrel(-dy))
            links.send(("woc",), theirs, theirs, dev(dc=1))

    def step_back(k, cc):
        if k == 0:
            present(cc)
        elif k < UP:

            @pl.when(z + k >= Z)
            def _():
                past([-k, k], cc)

            @pl.when((z >= k) & (z + k < Z))
            def _():
                past([-k], cc)

        else:

            @pl.when(z >= k)
            def _():
                past([-k], cc)

    def came(k):
        for d in [-k, k] if 0 < k < UP else [-k]:
            other_core(d)

    cut = (len(pieces) + 1) // 2
    for k in range(1, UP + 1):
        ring_step(k, pieces[:cut])
        step_back(k - 1, c)
        ring_step(k, pieces[cut:])
        to_core(-k)
        if k < UP:
            to_core(k)
        if k == UP:
            wo_forward()
        came(k - 1)
        step_back(k - 1, co)
        if k == 1:
            links.recv(("gz",), G.at[0 : Z - 1], dev(dz=1))
            CUM[...] = cumulative(G[...].reshape(Z * 8, GB)).reshape(Z, 8, GB)
    step_back(UP, c)
    came(UP)
    step_back(UP, co)

    for t in range(X):
        acc = ACC[t]
        o = (acc[:HEAD_DIM] / acc[HEAD_DIM : HEAD_DIM + 1]).astype(jnp.bfloat16)
        for yy in range(Y):
            part = o[:, yy * TB : (yy + 1) * TB]
            for h in range(2):
                OS[t, yy, :, h * TB : (h + 1) * TB] = part[h * HALF : (h + 1) * HALF]

    def at_rows(xx, yy):
        return AT.at[pl.ds(pl.multiple_of((yy * X + xx) * HALF, HALF), HALF), :]

    for dx, dy in plane:
        links.send(("o",), OS.at[xrel(dx), yrel(dy)], at_rows(x, y), dev(dx=dx, dy=dy))
    at_rows(x, y)[...] = OS[x, y]
    links.recv(("woc",), WO.at[:, 0 : wo_rows(X * Y), :], dev(dc=1))
    links.recv(("o",), AT.at[0 : len(plane) * HALF], dev(dx=1))

    attended = AT[...]
    for cc in range(C):
        for xx in range(X):
            block = (cc * X + xx) * Z * PR
            part = sum(
                jnp.dot(WO[h, block : block + Z * PR, :], attended, preferred_element_type=jnp.float32)[
                    :, h * TB : (h + 1) * TB
                ]
                for h in range(2)
            )
            for zz in range(Z):
                to = ((zz * X + xx) * C + cc) * PR
                PT[to : to + PR, 0:TB] = part[zz * PR : (zz + 1) * PR]
    out_ref[...] = rms_norm(PT[...].T[:TB], ogain_ref[...])
    links.drain(dev(dc=1))


def layer(dims, tokens, norm_gain, w_query, w_key, w_value, w_forget, forget_offset, w_out_t, out_gain):
    Z, X, C, Y = dims
    TB, D = tokens.shape
    PR, WC = w_query.shape
    GB = TB * Y
    HB = GB // 2
    LW = 3 * WC + LANES
    keys = Z * X * C * HB
    n_sems = 101
    vmem, smem = pl.BlockSpec(memory_space=pltpu.VMEM), pl.BlockSpec(memory_space=pltpu.SMEM)
    bf16, f32 = jnp.bfloat16, jnp.float32
    scratch = [
        pltpu.VMEM((Z, X * C * PR, LW), bf16),
        pltpu.VMEM((GB, D), bf16),
        pltpu.VMEM((2, D, D // 2), bf16),
        pltpu.VMEM((X, HB, LANES), bf16),
        pltpu.VMEM((X, 2, HEAD_DIM, HB), bf16),
        pltpu.VMEM((X, HEAD_DIM, GB), bf16),
        pltpu.VMEM((8, GB), f32),
        pltpu.VMEM((X, 8, GB), f32),
        pltpu.VMEM((8, GB), f32),
        pltpu.VMEM((8, GB), f32),
        pltpu.VMEM((Z, 8, GB), f32),
        pltpu.VMEM((Z, 8, GB), f32),
        pltpu.VMEM((keys, LANES), bf16),
        pltpu.VMEM((2, HEAD_DIM + 16, keys), bf16),
        pltpu.VMEM((X, HEAD_DIM, GB), bf16),
        pltpu.VMEM((X, LANES, 2 * GB), bf16),
        pltpu.VMEM((X, 1, GB), f32),
        pltpu.VMEM((X, HEAD_DIM + 16, GB), f32),
        pltpu.VMEM((X, Y, HEAD_DIM // 2, 2 * TB), bf16),
        pltpu.VMEM((D // 2, 2 * TB), bf16),
        pltpu.VMEM((D, LANES), f32),
        pltpu.VMEM((3, 2, 2 * HB, GB), f32),
        pltpu.VMEM((2, 4 * HB, GB), bf16),
        pltpu.VMEM((2, PR, WC // 2), bf16),
        pltpu.SemaphoreType.DMA((5,)),
        pltpu.SemaphoreType.DMA((n_sems,)),
    ]
    return pl.pallas_call(
        functools.partial(kernel, dims),
        out_shape=jax.ShapeDtypeStruct((TB, D), bf16),
        in_specs=[vmem] * 6 + [smem, vmem, vmem],
        out_specs=vmem,
        scratch_shapes=scratch,
        compiler_params=pltpu.CompilerParams(
            collective_id=0, has_side_effects=True, vmem_limit_bytes=56 * 1024 * 1024
        ),
    )(
        tokens,
        norm_gain.reshape(1, D),
        w_query,
        w_key,
        w_value,
        w_forget.T,
        forget_offset,
        w_out_t,
        out_gain.reshape(1, D),
    )


def sharded(mesh, dims):
    finer = Mesh(mesh.devices.reshape(*dims), AXES)
    sp = ("z", "x", "c")
    return jax.shard_map(
        functools.partial(layer, dims),
        mesh=finer,
        in_specs=(
            P(AXES, None),
            P(),
            P(sp, "y"),
            P(sp, "y"),
            P(sp, "y"),
            P(sp, "y"),
            P("y"),
            P(sp, "y"),
            P(),
        ),
        out_specs=P(AXES, None),
        check_vma=False,
    )


def solution(mesh):
    return sharded(mesh, (8, 4, 2, mesh.shape["tp"]))
```

```python
import functools
import math

import jax
import jax.numpy as jnp
from jax import lax
from jax.experimental import pallas as pl
from jax.experimental.pallas import tpu as pltpu
from jax.sharding import Mesh
from jax.sharding import PartitionSpec as P

HEAD_DIM = 64
AXES = ("z", "x", "c", "y")
MESH = pl.DeviceIdType.MESH
EPS = 1e-06
LOG2E = 1.4426950408889634
LOW = -1e30
LANES = 128


def rms_norm(floats, gain_row):
    scale_row = lax.rsqrt(jnp.mean(floats * floats, axis=-1, keepdims=True) + EPS)
    return (floats * scale_row * gain_row).astype(jnp.bfloat16)


def log_sigmoid(t):
    u = jnp.exp(-jnp.abs(t))
    series = u * (1.0 - u * (0.5 - u * (1.0 / 3.0 - u * 0.25)))
    return jnp.minimum(t, 0.0) - jnp.where(u < 0.01, series, jnp.log(1.0 + u))


class Links:
    def __init__(self, send_sems, recv_sems, counter):
        self.send_sems, self.recv_sems, self.counter = send_sems, recv_sems, counter
        self.ids, self.sent = {}, [0]
        self.most = counter.shape[0]

    def copy(self, key, src, dst, dev):
        return pltpu.make_async_remote_copy(
            src_ref=src,
            dst_ref=dst,
            send_sem=self.send_sems.at[len(self.sent) - 1],
            recv_sem=self.recv_sems.at[self.ids.setdefault(key, len(self.ids))],
            device_id=dev,
            device_id_type=MESH,
        )

    def send(self, key, src, dst, dev):
        rows = math.prod(src.shape) * src.dtype.itemsize // (2 * LANES)
        if self.sent[-1] + rows > self.most:
            self.sent.append(0)
        self.sent[-1] += rows
        self.copy(key, src, dst, dev).start()

    def recv(self, key, landed, dev):
        self.copy(key, landed, landed, dev).wait_recv()

    def drain(self, dev):
        for at, rows in enumerate(self.sent):
            view = self.counter.at[0:rows]
            pltpu.make_async_remote_copy(
                src_ref=view,
                dst_ref=view,
                send_sem=self.send_sems.at[at],
                recv_sem=self.recv_sems.at[0],
                device_id=dev,
                device_id_type=MESH,
            ).wait_send()


def kernel(
    dims,
    tokens_ref,
    gain_ref,
    wq_ref,
    wk_ref,
    wv_ref,
    wf_ref,
    off_ref,
    wo_ref,
    ogain_ref,
    out_ref,
    W,
    XN,
    WO,
    KS,
    VS,
    QS,
    GS,
    GX,
    GP,
    GPR,
    G,
    CUM,
    K,
    VT,
    QT,
    QB,
    M,
    ACC,
    OS,
    AT,
    PT,
    SC,
    PB,
    WO_OWN,
    send_sems,
    recv_sems,
):
    Z, X, C, Y = dims
    TB, D = tokens_ref.shape
    GB = TB * Y
    HB = GB // 2
    PR, WC = wo_ref.shape
    LW = W.shape[2]
    z, x, c, y = (lax.axis_index(a) for a in AXES)
    links = Links(send_sems, recv_sems, K)

    def dev(dz=0, dx=0, dc=0, dy=0):
        return {
            "z": lax.rem(z + (dz % Z), Z),
            "x": lax.rem(x + (dx % X), X),
            "c": lax.rem(c + (dc % C), C),
            "y": lax.rem(y + (dy % Y), Y),
        }

    def zrel(d):
        return lax.rem(z + (d % Z), Z)

    def xrel(d):
        return lax.rem(x + (d % X), X)

    def yrel(d):
        return lax.rem(y + (d % Y), Y)

    co = 1 - c
    plane = [(dx, dy) for dx in range(X) for dy in range(Y) if (dx, dy) != (0, 0)]
    far_first = sorted(range(1, Z), key=lambda d: -min(d, Z - d))
    near_first = [0] + far_first[::-1]
    x_near, y_near = ([1] if n == 2 else [1, -1] for n in (X, Y))

    barrier = pltpu.get_barrier_semaphore()
    greeted = (
        [dict(dx=dx, dy=dy) for dx, dy in plane] + [dict(dc=1)] + [dict(dz=d) for d in range(1, Z)]
    )
    for g in greeted:
        pl.semaphore_signal(barrier, inc=1, device_id=dev(**g), device_id_type=MESH)

    def w_rows(xx, cc):
        return pl.ds(pl.multiple_of((xx * C + cc) * PR, PR), PR)

    KVF, Q = (0, 2 * WC + LANES), (2 * WC + LANES, LW)
    mine = w_rows(x, c)
    W[z, mine, 0:WC] = wk_ref[...]
    W[z, mine, WC : 2 * WC] = wv_ref[...]
    W[z, mine, KVF[1] :] = wq_ref[...]
    PT[0:LANES] = jnp.zeros((LANES, LANES), jnp.float32)
    PT[0:X, 0:PR] = wf_ref[...].astype(jnp.float32)
    W[z, mine, 2 * WC : KVF[1]] = PT[0:LANES].T[:PR].astype(jnp.bfloat16)

    def t_rows(yy, lo=0, count=TB):
        return XN.at[pl.ds(pl.multiple_of(yy * TB + lo, 32), count), :]

    t_rows(y)[...] = rms_norm(tokens_ref[...].astype(jnp.float32), gain_ref[...])

    HALF = HEAD_DIM // 2
    WH = WC // 2

    def wo_columns(yy):
        return pl.ds(pl.multiple_of(yy * WH, WH), WH)

    def wo_block(cc, xx, zz, yy):
        row = ((cc * X + xx) * Z + zz) * PR
        return WO.at[:, pl.ds(pl.multiple_of(row, PR), PR), wo_columns(yy)]

    def wo_bundle(cc, xx, yy):
        row = (cc * X + xx) * Z * PR
        return WO.at[:, pl.ds(pl.multiple_of(row, PR), Z * PR), wo_columns(yy)]

    own_wo = wo_ref[...].astype(jnp.float32)
    for h in range(2):
        cols = [own_wo[:, i * HALF : (i + 1) * HALF] for i in range(h, 2 * X, 2)]
        WO_OWN[h] = jnp.concatenate(cols, axis=1).astype(jnp.bfloat16)
    wo_block(c, x, z, y)[...] = WO_OWN[...]
    pl.semaphore_wait(barrier, len(greeted))

    def w_unit(d, xx, cc, lanes):
        return W.at[zrel(d), w_rows(xx, cc), lanes[0] : lanes[1]]

    def w_bundle(xx, cc, lanes):
        return W.at[:, w_rows(xx, cc), lanes[0] : lanes[1]]

    def halves(lanes):
        middle = lanes[0] + -(-(lanes[1] - lanes[0]) // (2 * LANES)) * LANES
        return (lanes[0], middle), (middle, lanes[1])

    opposite = X > 2

    def fine_z(d):
        if d != 0:
            links.recv(("wz", d), w_unit(-d, x, c, KVF), dev(dz=-d))
        for dx in x_near:
            unit = w_unit(-d, x, c, KVF)
            links.send(("x1", d, dx), unit, unit, dev(dx=dx))

    def fine_x(d):
        for dx, part in zip(x_near, halves(KVF)):
            links.recv(("x1", d, dx), w_unit(-d, xrel(-dx), c, KVF), dev(dx=-dx))
            if opposite:
                unit = w_unit(-d, xrel(-dx), c, part)
                links.send(("x2", d, dx), unit, unit, dev(dx=dx))

    def fine_last(d):
        for dx, part in zip(x_near, halves(KVF)):
            links.recv(("x2", d, dx), w_unit(-d, xrel(2), c, part), dev(dx=-dx))
        unit = w_unit(-d, xrel(2), c, KVF)
        links.send(("wc", KVF), unit, unit, dev(dc=1))

    def to_other_core(xx, lanes):
        view = w_bundle(xx, c, lanes)
        links.send(("wc", lanes), view, view, dev(dc=1))

    def core_last(lanes):
        links.recv(("wc", lanes), W.at[:, 0 : X * PR, lanes[0] : lanes[1]], dev(dc=1))

    for lanes in (KVF, Q):
        for d in far_first:
            unit = w_unit(0, x, c, lanes)
            links.send(("wz", d if lanes == KVF else Q), unit, unit, dev(dz=d))
    for dy in y_near:
        links.send(("tok", dy), t_rows(y), t_rows(y), dev(dy=dy))
    for d in far_first:
        links.send(("woz",), WO_OWN, wo_block(c, x, z, y), dev(dz=d))

    QB[...] = jnp.zeros_like(QB)
    VT[:, HEAD_DIM:, :] = jnp.ones((2, VT.shape[1] - HEAD_DIM, VT.shape[2]), jnp.bfloat16)
    M[...] = jnp.full(M.shape, LOW, jnp.float32)
    ACC[...] = jnp.zeros_like(ACC)

    for d in near_first:
        fine_z(d)
    to_other_core(x, KVF)
    for dy, lo in zip(y_near, (0, TB // 2)):
        links.recv(("tok", dy), t_rows(yrel(-dy)), dev(dy=-dy))
        if Y > 2:
            part = t_rows(yrel(-dy), lo, TB // 2)
            links.send(("tok2", dy), part, part, dev(dy=dy))
    for d in near_first:
        fine_x(d)
    for dx in x_near:
        to_other_core(xrel(-dx), KVF)
    links.recv(("wz", Q), W.at[0 : Z - 1, 0:PR, Q[0] : Q[1]], dev(dz=1))
    for dx in x_near:
        view = w_bundle(x, c, Q)
        links.send(("x1", Q, dx), view, view, dev(dx=dx))
    if opposite:
        for d in near_first:
            fine_last(d)
    for dx, part in zip(x_near, halves(Q)):
        links.recv(("x1", Q, dx), w_bundle(xrel(-dx), c, Q), dev(dx=-dx))
        if opposite:
            view = w_bundle(xrel(-dx), c, part)
            links.send(("x2", Q, dx), view, view, dev(dx=dx))
    for dx in [0] + x_near:
        to_other_core(xrel(-dx), Q)
    if Y > 2:
        for dy, lo in zip(y_near, (0, TB // 2)):
            links.recv(("tok2", dy), t_rows(yrel(2), lo, TB // 2), dev(dy=-dy))
    core_last(KVF)

    rows = XN[...]

    def project(lo, count):
        weight = W[:, :, lo : lo + count].reshape(D, count)
        return jnp.dot(rows, weight, preferred_element_type=jnp.float32)

    def slot(cc, zz, xx):
        return ((cc * Z + zz) * X + xx) * HB

    def k_block(cc, zz, xx):
        return K.at[pl.ds(pl.multiple_of(slot(cc, zz, xx), LANES), HB), :]

    def v_block(cc, zz, xx):
        return VT.at[:, 0:HEAD_DIM, pl.ds(pl.multiple_of(slot(cc, zz, xx), LANES), HB)]

    gates = project(2 * WC, LANES).T[:8]
    head_row = lax.broadcasted_iota(jnp.int32, gates.shape, 0)
    offset = jnp.zeros_like(gates)
    for h in range(X):
        offset = jnp.where(head_row == h, off_ref[h], offset)
    GS[...] = log_sigmoid(gates + offset + math.log(GB * Z * X * C))
    for dx in range(1, X):
        links.send(("g",), GS, GX.at[x], dev(dx=dx))
    GX[x] = GS[...]
    k_all = project(0, WC)
    for h in range(X):
        kh = k_all[:, h * HEAD_DIM : (h + 1) * HEAD_DIM]
        KS[h] = jnp.concatenate([kh[:HB], kh[HB:]], axis=1).astype(jnp.bfloat16)
    for dx in range(1, X):
        links.send(("kv", dx), KS.at[xrel(dx)], k_block(c, z, x), dev(dx=dx))
    if opposite:
        for dx, part in zip(x_near, halves(Q)):
            links.recv(("x2", Q, dx), w_bundle(xrel(2), c, part), dev(dx=-dx))
        to_other_core(xrel(2), Q)
    v_all = project(WC, WC).T
    for h in range(X):
        vh = v_all[h * HEAD_DIM : (h + 1) * HEAD_DIM].astype(jnp.bfloat16)
        VS[h, 0] = vh[:, :HB]
        VS[h, 1] = vh[:, HB:]
    for dx in range(1, X):
        links.send(("kv", dx), VS.at[xrel(dx)], v_block(c, z, x), dev(dx=dx))
    k_block(c, z, x)[...] = KS[x]
    v_block(c, z, x)[...] = VS[x]

    UP = DN = Z // 2

    def goes(way, a, k):
        return k < UP or (k == UP and (a == 0) == (way == "up"))

    def bundle(zz, cc):
        at = pl.multiple_of(slot(cc, zz, 0), LANES)
        return K.at[pl.ds(at, X * HB), :], VT.at[:, 0:HEAD_DIM, pl.ds(at, X * HB)]

    def piece(zz, dx):
        return k_block(c, zz, xrel(-dx)), v_block(c, zz, xrel(-dx))

    WAYS = (("up", 1), ("dn", -1))
    pieces = [0] + ([1, X - 1] if X > 2 else [1]) + list(range(2, X - 1))

    def ring_start(dx):
        for a, view in enumerate(piece(z, dx)):
            for way, sign in WAYS:
                if goes(way, a, 1):
                    links.send((way, 1, dx), view, view, dev(dz=sign))

    def to_core(d):
        for view in bundle(zrel(d), c):
            links.send(("core", d % Z), view, view, dev(dc=1))

    def ring_step(k, some):
        for dx in some:
            for way, sign in WAYS:
                arrays = [a for a in range(2) if goes(way, a, k)]
                links.recv((way, k, dx), K.at[0 : len(arrays) * HB], dev(dz=-sign))
                for a in arrays:
                    if goes(way, a, k + 1):
                        view = piece(zrel(-sign * k), dx)[a]
                        links.send((way, k + 1, dx), view, view, dev(dz=sign))

    def other_core(d):
        links.recv(("core", d % Z), K.at[0 : 2 * X * HB], dev(dc=1))

    ring_start(0)
    core_last(Q)
    q_all = project(KVF[1], WC)
    q_all = q_all.astype(jnp.bfloat16).astype(jnp.float32) * (HEAD_DIM**-0.5 * LOG2E)
    q_all = q_all.T
    for h in range(X):
        QS[h] = q_all[h * HEAD_DIM : (h + 1) * HEAD_DIM].astype(jnp.bfloat16)
    for dx in range(1, X):
        links.send(("q",), QS.at[xrel(dx)], QT.at[x], dev(dx=dx))
    QT[x] = QS[x]

    links.recv(("g",), GX.at[0 : X - 1], dev(dx=1))
    row8 = lax.broadcasted_iota(jnp.int32, (8, GB), 0)
    own_gates = jnp.zeros((8, GB), jnp.float32)
    for sx in range(X):
        picked = jnp.sum(jnp.where(row8 == x, GX[sx], 0.0), axis=0, keepdims=True)
        own_gates = jnp.where(row8 == sx, picked, own_gates)
    GP[...] = own_gates
    links.send(("gp",), GP, GPR, dev(dc=1))
    def next_piece(dx):
        links.recv(("kv", dx), K.at[0 : 2 * HB], dev(dx=-dx))
        ring_start(dx)

    for dx in pieces[1:-1]:
        next_piece(dx)
    links.recv(("gp",), GPR, dev(dc=1))
    theirs = GPR[...]
    chip_gates = jnp.zeros((8, GB), jnp.float32)
    for sx in range(X):
        a, b = own_gates[sx : sx + 1], theirs[sx : sx + 1]
        chip_gates = jnp.where(row8 == 2 * sx, jnp.where(c == 0, a, b), chip_gates)
        chip_gates = jnp.where(row8 == 2 * sx + 1, jnp.where(c == 0, b, a), chip_gates)
    G[z] = chip_gates
    for d in far_first:
        links.send(("gz",), G.at[z], G.at[z], dev(dz=d))
    for dx in pieces[-1:]:
        next_piece(dx)
    to_core(0)

    links.recv(("q",), QT.at[0 : X - 1], dev(dx=1))
    for sx in range(X):
        QB[sx, 0:HEAD_DIM, 0:GB] = QT[sx]
        QB[sx, HEAD_DIM:, GB:] = QT[sx]
    links.recv(("woz",), WO.at[:, 0 : (Z - 1) * PR, 0:WH], dev(dz=1))
    own = wo_bundle(c, x, y)
    for dx, dy in plane:
        links.send(("woxy",), own, own, dev(dx=dx, dy=dy))
    links.send(("woc",), own, own, dev(dc=1))

    def cumulative(block):
        n = block.shape[0]
        lane = lax.broadcasted_iota(jnp.int32, block.shape, 1)
        step = 1
        while step < GB:
            block = block + jnp.where(lane >= step, pltpu.roll(block, step, 1), 0.0)
            step *= 2
        total = jnp.broadcast_to(block[:, GB - 1 :], (n, LANES))
        row = lax.broadcasted_iota(jnp.int32, total.shape, 0)
        before = jnp.where(row >= 1, pltpu.roll(total, 1, 0), 0.0)
        step = 1
        while step < n:
            before = before + jnp.where(row >= step, pltpu.roll(before, step, 0), 0.0)
            step *= 2
        return (block + before[:, 0:1]) * LOG2E

    def query_sums(block):
        return [
            jnp.sum(jnp.where(row8 == 2 * sx + c, block, 0.0), axis=0, keepdims=True)
            for sx in range(X)
        ]

    def key_sums(block, cc):
        block = jnp.where(cc == 0, block, pltpu.roll(block, 7, 0))
        both = jnp.concatenate([block[:, :HB], block[:, HB:]], axis=0)
        both = jnp.concatenate([both, jnp.zeros((LANES - 16, HB), jnp.float32)], axis=0)
        return both.T

    def attend(items, cum_q):
        AHEAD, SOFT = 3, 1
        n_s, n_p = AHEAD - SOFT + 1, SOFT + 1
        best, rescale, loaded = {}, {}, {}

        def prepared(table, at, pair):
            key = (id(table), pair)
            if key not in loaded:
                even, odd = 4 * pair, 4 * pair + 2
                b0 = [table[:, even : even + 1], table[:, odd : odd + 1]]
                b1 = [table[:, 8 + even : 9 + even], table[:, 8 + odd : 9 + odd]]
                start = pl.multiple_of(at + pair * 2 * HB, 2 * HB)
                loaded[key] = jnp.concatenate(b0, axis=0), jnp.concatenate(b1, axis=0), start
            return loaded[key]

        def scores(j):
            table, at, pair, t, mask = items[j]
            b0, b1, start = prepared(table, at, pair)
            s = jnp.dot(K[pl.ds(start, 2 * HB), :], QB[t], preferred_element_type=jnp.float32)
            s0, s1 = s[:, :GB] - b0, s[:, GB:] - b1
            if mask is not None:
                s0, s1 = mask(s0, 0, t), mask(s1, 1, t)
            SC[j % n_s, 0], SC[j % n_s, 1] = s0, s1
            best[j] = jnp.maximum(jnp.max(s0, axis=0, keepdims=True), jnp.max(s1, axis=0, keepdims=True))

        def softmax(j):
            t = items[j][3]
            old = M[t]
            new = jnp.maximum(old, best[j] + cum_q[t])
            rescale[j] = jnp.exp2(old - new)
            M[t] = new
            shift = new - cum_q[t]
            PB[j % n_p, : 2 * HB] = jnp.exp2(SC[j % n_s, 0] - shift).astype(jnp.bfloat16)
            PB[j % n_p, 2 * HB :] = jnp.exp2(SC[j % n_s, 1] - shift).astype(jnp.bfloat16)

        def weigh(j):
            table, at, pair, t, _ = items[j]
            start = prepared(table, at, pair)[2]
            v = jnp.concatenate(
                [VT[0, :, pl.ds(start, 2 * HB)], VT[1, :, pl.ds(start, 2 * HB)]], axis=1
            )
            ACC[t] = ACC[t] * rescale[j] + jnp.dot(
                v, PB[j % n_p], preferred_element_type=jnp.float32
            )

        for j in range(-AHEAD, len(items)):
            if 0 <= j + AHEAD < len(items):
                scores(j + AHEAD)
            if j >= 0:
                weigh(j)
            if 0 <= j + SOFT < len(items):
                softmax(j + SOFT)

    cum_here = cumulative(G[z])
    cum_q_here = query_sums(cum_here)

    def present(cc):
        def masked(pair):
            def mask(s, which, t):
                r = lax.broadcasted_iota(jnp.int32, s.shape, 0)
                first = 4 * pair + cc
                key = jnp.where(r < HB, first * GB + r, (first + 2) * GB + r - HB) + which * HB
                query = (2 * t + c) * GB + lax.broadcasted_iota(jnp.int32, s.shape, 1)
                return jnp.where(key <= query, s, LOW)

            return mask

        table = key_sums(cum_here, cc)
        items = [
            (table, slot(cc, z, 0), pair, t, masked(pair) if t <= 2 * pair + 1 else None)
            for pair in range(X // 2)
            for t in range(2 * pair, X)
        ]
        attend(items, cum_q_here)

    def past(ds, cc):
        items = []
        for d in ds:
            zz = zrel(d)
            table = key_sums(CUM[zz], cc)
            items += [
                (table, slot(cc, zz, 0), pair, t, None) for pair in range(X // 2) for t in range(X)
            ]
        attend(items, query_sums(CUM[z]))

    def wo_rows(bundles):
        return bundles * Z * PR * WH // WO.shape[2]

    def wo_forward():
        links.recv(("woxy",), WO.at[:, 0 : wo_rows(len(plane)), :], dev(dx=1))
        for dx, dy in plane:
            theirs = wo_bundle(c, xrel(-dx), yrel(-dy))
            links.send(("woc",), theirs, theirs, dev(dc=1))

    def step_back(k, cc):
        if k == 0:
            present(cc)
        elif k < UP:

            @pl.when(z + k >= Z)
            def _():
                past([-k, k], cc)

            @pl.when((z >= k) & (z + k < Z))
            def _():
                past([-k], cc)

        else:

            @pl.when(z >= k)
            def _():
                past([-k], cc)

    def came(k):
        for d in [-k, k] if 0 < k < UP else [-k]:
            other_core(d)

    cut = (len(pieces) + 1) // 2
    for k in range(1, UP + 1):
        ring_step(k, pieces[:cut])
        step_back(k - 1, c)
        ring_step(k, pieces[cut:])
        to_core(-k)
        if k < UP:
            to_core(k)
        if k == UP:
            wo_forward()
        came(k - 1)
        step_back(k - 1, co)
        if k == 1:
            links.recv(("gz",), G.at[0 : Z - 1], dev(dz=1))
            CUM[...] = cumulative(G[...].reshape(Z * 8, GB)).reshape(Z, 8, GB)
    step_back(UP, c)
    came(UP)
    step_back(UP, co)

    for t in range(X):
        acc = ACC[t]
        o = (acc[:HEAD_DIM] / acc[HEAD_DIM : HEAD_DIM + 1]).astype(jnp.bfloat16)
        for yy in range(Y):
            part = o[:, yy * TB : (yy + 1) * TB]
            for h in range(2):
                OS[t, yy, :, h * TB : (h + 1) * TB] = part[h * HALF : (h + 1) * HALF]

    def at_rows(xx, yy):
        return AT.at[pl.ds(pl.multiple_of((yy * X + xx) * HALF, HALF), HALF), :]

    for dx, dy in plane:
        links.send(("o",), OS.at[xrel(dx), yrel(dy)], at_rows(x, y), dev(dx=dx, dy=dy))
    at_rows(x, y)[...] = OS[x, y]
    links.recv(("woc",), WO.at[:, 0 : wo_rows(X * Y), :], dev(dc=1))
    links.recv(("o",), AT.at[0 : len(plane) * HALF], dev(dx=1))

    attended = AT[...]
    for cc in range(C):
        for xx in range(X):
            block = (cc * X + xx) * Z * PR
            part = sum(
                jnp.dot(WO[h, block : block + Z * PR, :], attended, preferred_element_type=jnp.float32)[
                    :, h * TB : (h + 1) * TB
                ]
                for h in range(2)
            )
            for zz in range(Z):
                to = ((zz * X + xx) * C + cc) * PR
                PT[to : to + PR, 0:TB] = part[zz * PR : (zz + 1) * PR]
    out_ref[...] = rms_norm(PT[...].T[:TB], ogain_ref[...])
    links.drain(dev(dc=1))


def layer(dims, tokens, norm_gain, w_query, w_key, w_value, w_forget, forget_offset, w_out_t, out_gain):
    Z, X, C, Y = dims
    TB, D = tokens.shape
    PR, WC = w_query.shape
    GB = TB * Y
    HB = GB // 2
    LW = 3 * WC + LANES
    keys = Z * X * C * HB
    n_sems = 101
    vmem, smem = pl.BlockSpec(memory_space=pltpu.VMEM), pl.BlockSpec(memory_space=pltpu.SMEM)
    bf16, f32 = jnp.bfloat16, jnp.float32
    scratch = [
        pltpu.VMEM((Z, X * C * PR, LW), bf16),
        pltpu.VMEM((GB, D), bf16),
        pltpu.VMEM((2, D, D // 2), bf16),
        pltpu.VMEM((X, HB, LANES), bf16),
        pltpu.VMEM((X, 2, HEAD_DIM, HB), bf16),
        pltpu.VMEM((X, HEAD_DIM, GB), bf16),
        pltpu.VMEM((8, GB), f32),
        pltpu.VMEM((X, 8, GB), f32),
        pltpu.VMEM((8, GB), f32),
        pltpu.VMEM((8, GB), f32),
        pltpu.VMEM((Z, 8, GB), f32),
        pltpu.VMEM((Z, 8, GB), f32),
        pltpu.VMEM((keys, LANES), bf16),
        pltpu.VMEM((2, HEAD_DIM + 16, keys), bf16),
        pltpu.VMEM((X, HEAD_DIM, GB), bf16),
        pltpu.VMEM((X, LANES, 2 * GB), bf16),
        pltpu.VMEM((X, 1, GB), f32),
        pltpu.VMEM((X, HEAD_DIM + 16, GB), f32),
        pltpu.VMEM((X, Y, HEAD_DIM // 2, 2 * TB), bf16),
        pltpu.VMEM((D // 2, 2 * TB), bf16),
        pltpu.VMEM((D, LANES), f32),
        pltpu.VMEM((3, 2, 2 * HB, GB), f32),
        pltpu.VMEM((2, 4 * HB, GB), bf16),
        pltpu.VMEM((2, PR, WC // 2), bf16),
        pltpu.SemaphoreType.DMA((5,)),
        pltpu.SemaphoreType.DMA((n_sems,)),
    ]
    return pl.pallas_call(
        functools.partial(kernel, dims),
        out_shape=jax.ShapeDtypeStruct((TB, D), bf16),
        in_specs=[vmem] * 6 + [smem, vmem, vmem],
        out_specs=vmem,
        scratch_shapes=scratch,
        compiler_params=pltpu.CompilerParams(
            collective_id=0, has_side_effects=True, vmem_limit_bytes=56 * 1024 * 1024
        ),
    )(
        tokens,
        norm_gain.reshape(1, D),
        w_query,
        w_key,
        w_value,
        w_forget.T,
        forget_offset,
        w_out_t,
        out_gain.reshape(1, D),
    )


def sharded(mesh, dims):
    finer = Mesh(mesh.devices.reshape(*dims), AXES)
    sp = ("z", "x", "c")
    return jax.shard_map(
        functools.partial(layer, dims),
        mesh=finer,
        in_specs=(
            P(AXES, None),
            P(),
            P(sp, "y"),
            P(sp, "y"),
            P(sp, "y"),
            P(sp, "y"),
            P("y"),
            P(sp, "y"),
            P(),
        ),
        out_specs=P(AXES, None),
        check_vma=False,
    )


def solution(mesh):
    return sharded(mesh, (8, 4, 2, mesh.shape["tp"]))
```

```python
import functools
import math

import jax
import jax.numpy as jnp
from jax import lax
from jax.experimental import pallas as pl
from jax.experimental.pallas import tpu as pltpu
from jax.sharding import Mesh
from jax.sharding import PartitionSpec as P

HEAD_DIM = 64
AXES = ("z", "x", "c", "y")
MESH = pl.DeviceIdType.MESH
EPS = 1e-06
LOG2E = 1.4426950408889634
LOW = -1e30
LANES = 128


def rms_norm(floats, gain_row):
    scale_row = lax.rsqrt(jnp.mean(floats * floats, axis=-1, keepdims=True) + EPS)
    return (floats * scale_row * gain_row).astype(jnp.bfloat16)


def log_sigmoid(t):
    u = jnp.exp(-jnp.abs(t))
    series = u * (1.0 - u * (0.5 - u * (1.0 / 3.0 - u * 0.25)))
    return jnp.minimum(t, 0.0) - jnp.where(u < 0.01, series, jnp.log(1.0 + u))


class Links:
    def __init__(self, send_sems, recv_sems, counter):
        self.send_sems, self.recv_sems, self.counter = send_sems, recv_sems, counter
        self.ids, self.sent = {}, [0]
        self.most = counter.shape[0]

    def copy(self, key, src, dst, dev):
        return pltpu.make_async_remote_copy(
            src_ref=src,
            dst_ref=dst,
            send_sem=self.send_sems.at[len(self.sent) - 1],
            recv_sem=self.recv_sems.at[self.ids.setdefault(key, len(self.ids))],
            device_id=dev,
            device_id_type=MESH,
        )

    def send(self, key, src, dst, dev):
        rows = math.prod(src.shape) * src.dtype.itemsize // (2 * LANES)
        if self.sent[-1] + rows > self.most:
            self.sent.append(0)
        self.sent[-1] += rows
        self.copy(key, src, dst, dev).start()

    def recv(self, key, landed, dev):
        self.copy(key, landed, landed, dev).wait_recv()

    def drain(self, dev):
        for at, rows in enumerate(self.sent):
            view = self.counter.at[0:rows]
            pltpu.make_async_remote_copy(
                src_ref=view,
                dst_ref=view,
                send_sem=self.send_sems.at[at],
                recv_sem=self.recv_sems.at[0],
                device_id=dev,
                device_id_type=MESH,
            ).wait_send()


def kernel(
    dims,
    tokens_hbm,
    gain_hbm,
    wq_hbm,
    wk_hbm,
    wv_hbm,
    wf_hbm,
    off_ref,
    wo_hbm,
    ogain_hbm,
    out_ref,
    W,
    XN,
    WO,
    KS,
    VS,
    QS,
    GS,
    GX,
    GP,
    GPR,
    G,
    CUM,
    K,
    VT,
    QT,
    QB,
    M,
    ACC,
    OS,
    AT,
    PT,
    SC,
    PB,
    WO_OWN,
    tokens_ref,
    gain_ref,
    wq_ref,
    wk_ref,
    wv_ref,
    wf_ref,
    wo_ref,
    ogain_ref,
    in_sems,
    send_sems,
    recv_sems,
):
    Z, X, C, Y = dims
    TB, D = tokens_hbm.shape
    GB = TB * Y
    HB = GB // 2
    PR, WC = wo_hbm.shape
    LW = W.shape[2]
    z, x, c, y = (lax.axis_index(a) for a in AXES)
    links = Links(send_sems, recv_sems, K)

    def dev(dz=0, dx=0, dc=0, dy=0):
        return {
            "z": lax.rem(z + (dz % Z), Z),
            "x": lax.rem(x + (dx % X), X),
            "c": lax.rem(c + (dc % C), C),
            "y": lax.rem(y + (dy % Y), Y),
        }

    def zrel(d):
        return lax.rem(z + (d % Z), Z)

    def xrel(d):
        return lax.rem(x + (d % X), X)

    def yrel(d):
        return lax.rem(y + (d % Y), Y)

    co = 1 - c
    plane = [(dx, dy) for dx in range(X) for dy in range(Y) if (dx, dy) != (0, 0)]
    plane.sort(key=lambda at: -min(at[0], X - at[0]) - min(at[1], Y - at[1]))
    x_far = sorted(range(1, X), key=lambda d: -min(d, X - d))
    far_first = sorted(range(1, Z), key=lambda d: -min(d, Z - d))
    near_first = [0] + far_first[::-1]
    x_near, y_near = ([1] if n == 2 else [1, -1] for n in (X, Y))

    barrier = pltpu.get_barrier_semaphore()
    greeted = (
        [dict(dx=dx, dy=dy) for dx, dy in plane] + [dict(dc=1)] + [dict(dz=d) for d in range(1, Z)]
    )
    for g in greeted:
        pl.semaphore_signal(barrier, inc=1, device_id=dev(**g), device_id_type=MESH)

    operands = (
        (wk_hbm, wk_ref),
        (wv_hbm, wv_ref),
        (wq_hbm, wq_ref),
        (wf_hbm, wf_ref),
        (tokens_hbm, tokens_ref),
        (gain_hbm, gain_ref),
        (wo_hbm, wo_ref),
        (ogain_hbm, ogain_ref),
    )
    fetches = [
        pltpu.make_async_copy(src, dst, in_sems.at[i]) for i, (src, dst) in enumerate(operands)
    ]
    for fetch in fetches:
        fetch.start()
    for fetch in fetches:
        fetch.wait()

    def w_rows(xx, cc):
        return pl.ds(pl.multiple_of((xx * C + cc) * PR, PR), PR)

    KVF, Q = (0, 2 * WC + LANES), (2 * WC + LANES, LW)
    mine = w_rows(x, c)
    W[z, mine, 0:WC] = wk_ref[...]
    W[z, mine, WC : 2 * WC] = wv_ref[...]
    W[z, mine, KVF[1] :] = wq_ref[...]
    PT[0:LANES] = jnp.zeros((LANES, LANES), jnp.float32)
    PT[0:X, 0:PR] = wf_ref[...].astype(jnp.float32)
    W[z, mine, 2 * WC : KVF[1]] = PT[0:LANES].T[:PR].astype(jnp.bfloat16)

    def t_rows(yy, lo=0, count=TB):
        return XN.at[pl.ds(pl.multiple_of(yy * TB + lo, 32), count), :]

    t_rows(y)[...] = rms_norm(tokens_ref[...].astype(jnp.float32), gain_ref[...])

    HALF = HEAD_DIM // 2
    WH = WC // 2

    def wo_columns(yy):
        return pl.ds(pl.multiple_of(yy * WH, WH), WH)

    def wo_block(cc, xx, zz, yy):
        row = ((cc * X + xx) * Z + zz) * PR
        return WO.at[:, pl.ds(pl.multiple_of(row, PR), PR), wo_columns(yy)]

    def wo_bundle(cc, xx, yy):
        row = (cc * X + xx) * Z * PR
        return WO.at[:, pl.ds(pl.multiple_of(row, PR), Z * PR), wo_columns(yy)]

    own_wo = wo_ref[...].astype(jnp.float32)
    for h in range(2):
        cols = [own_wo[:, i * HALF : (i + 1) * HALF] for i in range(h, 2 * X, 2)]
        WO_OWN[h] = jnp.concatenate(cols, axis=1).astype(jnp.bfloat16)
    wo_block(c, x, z, y)[...] = WO_OWN[...]
    pl.semaphore_wait(barrier, len(greeted))

    def w_unit(d, xx, cc, lanes):
        return W.at[zrel(d), w_rows(xx, cc), lanes[0] : lanes[1]]

    def w_bundle(xx, cc, lanes):
        return W.at[:, w_rows(xx, cc), lanes[0] : lanes[1]]

    def halves(lanes):
        middle = lanes[0] + -(-(lanes[1] - lanes[0]) // (2 * LANES)) * LANES
        return (lanes[0], middle), (middle, lanes[1])

    opposite = X > 2

    def fine_z(d):
        if d != 0:
            links.recv(("wz", d), w_unit(-d, x, c, KVF), dev(dz=-d))
        for dx in x_near:
            unit = w_unit(-d, x, c, KVF)
            links.send(("x1", d, dx), unit, unit, dev(dx=dx))

    def fine_x(d):
        for dx, part in zip(x_near, halves(KVF)):
            links.recv(("x1", d, dx), w_unit(-d, xrel(-dx), c, KVF), dev(dx=-dx))
            if opposite:
                unit = w_unit(-d, xrel(-dx), c, part)
                links.send(("x2", d, dx), unit, unit, dev(dx=dx))

    def fine_last(d):
        for dx, part in zip(x_near, halves(KVF)):
            links.recv(("x2", d, dx), w_unit(-d, xrel(2), c, part), dev(dx=-dx))
        unit = w_unit(-d, xrel(2), c, KVF)
        links.send(("wc", KVF), unit, unit, dev(dc=1))

    def to_other_core(xx, lanes):
        view = w_bundle(xx, c, lanes)
        links.send(("wc", lanes), view, view, dev(dc=1))

    def core_last(lanes):
        links.recv(("wc", lanes), W.at[:, 0 : X * PR, lanes[0] : lanes[1]], dev(dc=1))

    for lanes in (KVF, Q):
        for d in far_first:
            unit = w_unit(0, x, c, lanes)
            links.send(("wz", d if lanes == KVF else Q), unit, unit, dev(dz=d))
    for dy in y_near:
        links.send(("tok", dy), t_rows(y), t_rows(y), dev(dy=dy))
    for d in far_first:
        links.send(("woz",), WO_OWN, wo_block(c, x, z, y), dev(dz=d))

    QB[...] = jnp.zeros_like(QB)
    VT[:, HEAD_DIM:, :] = jnp.ones((2, VT.shape[1] - HEAD_DIM, VT.shape[2]), jnp.bfloat16)
    M[...] = jnp.full(M.shape, LOW, jnp.float32)
    ACC[...] = jnp.zeros_like(ACC)

    for d in near_first:
        fine_z(d)
    to_other_core(x, KVF)
    for dy, lo in zip(y_near, (0, TB // 2)):
        links.recv(("tok", dy), t_rows(yrel(-dy)), dev(dy=-dy))
        if Y > 2:
            part = t_rows(yrel(-dy), lo, TB // 2)
            links.send(("tok2", dy), part, part, dev(dy=dy))
    for d in near_first:
        fine_x(d)
    for dx in x_near:
        to_other_core(xrel(-dx), KVF)
    links.recv(("wz", Q), W.at[0 : Z - 1, 0:PR, Q[0] : Q[1]], dev(dz=1))
    for dx in x_near:
        view = w_bundle(x, c, Q)
        links.send(("x1", Q, dx), view, view, dev(dx=dx))
    if opposite:
        for d in near_first:
            fine_last(d)
    for dx, part in zip(x_near, halves(Q)):
        links.recv(("x1", Q, dx), w_bundle(xrel(-dx), c, Q), dev(dx=-dx))
        if opposite:
            view = w_bundle(xrel(-dx), c, part)
            links.send(("x2", Q, dx), view, view, dev(dx=dx))
    for dx in [0] + x_near:
        to_other_core(xrel(-dx), Q)
    if Y > 2:
        for dy, lo in zip(y_near, (0, TB // 2)):
            links.recv(("tok2", dy), t_rows(yrel(2), lo, TB // 2), dev(dy=-dy))
    core_last(KVF)

    rows = XN[...]

    def project(lo, count):
        weight = W[:, :, lo : lo + count].reshape(D, count)
        return jnp.dot(rows, weight, preferred_element_type=jnp.float32)

    def slot(cc, zz, xx):
        return ((cc * Z + zz) * X + xx) * HB

    def k_block(cc, zz, xx):
        return K.at[pl.ds(pl.multiple_of(slot(cc, zz, xx), LANES), HB), :]

    def v_block(cc, zz, xx):
        return VT.at[:, 0:HEAD_DIM, pl.ds(pl.multiple_of(slot(cc, zz, xx), LANES), HB)]

    gates = project(2 * WC, LANES).T[:8]
    head_row = lax.broadcasted_iota(jnp.int32, gates.shape, 0)
    offset = jnp.zeros_like(gates)
    for h in range(X):
        offset = jnp.where(head_row == h, off_ref[h], offset)
    GS[...] = log_sigmoid(gates + offset + math.log(GB * Z * X * C))
    for dx in x_far:
        links.send(("g",), GS, GX.at[x], dev(dx=dx))
    GX[x] = GS[...]
    k_all = project(0, WC)
    for h in range(X):
        kh = k_all[:, h * HEAD_DIM : (h + 1) * HEAD_DIM]
        KS[h] = jnp.concatenate([kh[:HB], kh[HB:]], axis=1).astype(jnp.bfloat16)
    for dx in range(1, X):
        links.send(("kv", dx), KS.at[xrel(dx)], k_block(c, z, x), dev(dx=dx))
    if opposite:
        for dx, part in zip(x_near, halves(Q)):
            links.recv(("x2", Q, dx), w_bundle(xrel(2), c, part), dev(dx=-dx))
        to_other_core(xrel(2), Q)
    v_all = project(WC, WC).T
    for h in range(X):
        vh = v_all[h * HEAD_DIM : (h + 1) * HEAD_DIM].astype(jnp.bfloat16)
        VS[h, 0] = vh[:, :HB]
        VS[h, 1] = vh[:, HB:]
    for dx in range(1, X):
        links.send(("kv", dx), VS.at[xrel(dx)], v_block(c, z, x), dev(dx=dx))
    k_block(c, z, x)[...] = KS[x]
    v_block(c, z, x)[...] = VS[x]

    UP = DN = Z // 2

    def goes(way, a, k):
        return k < UP or (k == UP and (a == 0) == (way == "up"))

    def bundle(zz, cc):
        at = pl.multiple_of(slot(cc, zz, 0), LANES)
        return K.at[pl.ds(at, X * HB), :], VT.at[:, 0:HEAD_DIM, pl.ds(at, X * HB)]

    def piece(zz, dx):
        return k_block(c, zz, xrel(-dx)), v_block(c, zz, xrel(-dx))

    WAYS = (("up", 1), ("dn", -1))
    pieces = [0] + ([1, X - 1] if X > 2 else [1]) + list(range(2, X - 1))

    def ring_start(dx):
        for a, view in enumerate(piece(z, dx)):
            for way, sign in WAYS:
                if goes(way, a, 1):
                    links.send((way, 1, dx), view, view, dev(dz=sign))

    def to_core(d):
        for view in bundle(zrel(d), c):
            links.send(("core", d % Z), view, view, dev(dc=1))

    def ring_step(k, some):
        for dx in some:
            for way, sign in WAYS:
                arrays = [a for a in range(2) if goes(way, a, k)]
                links.recv((way, k, dx), K.at[0 : len(arrays) * HB], dev(dz=-sign))
                for a in arrays:
                    if goes(way, a, k + 1):
                        view = piece(zrel(-sign * k), dx)[a]
                        links.send((way, k + 1, dx), view, view, dev(dz=sign))

    def other_core(d):
        links.recv(("core", d % Z), K.at[0 : 2 * X * HB], dev(dc=1))

    ring_start(0)
    core_last(Q)
    q_all = project(KVF[1], WC)
    q_all = q_all.astype(jnp.bfloat16).astype(jnp.float32) * (HEAD_DIM**-0.5 * LOG2E)
    q_all = q_all.T
    for h in range(X):
        QS[h] = q_all[h * HEAD_DIM : (h + 1) * HEAD_DIM].astype(jnp.bfloat16)
    for dx in x_far:
        links.send(("q",), QS.at[xrel(dx)], QT.at[x], dev(dx=dx))
    QT[x] = QS[x]

    links.recv(("g",), GX.at[0 : X - 1], dev(dx=1))
    row8 = lax.broadcasted_iota(jnp.int32, (8, GB), 0)
    own_gates = jnp.zeros((8, GB), jnp.float32)
    for sx in range(X):
        picked = jnp.sum(jnp.where(row8 == x, GX[sx], 0.0), axis=0, keepdims=True)
        own_gates = jnp.where(row8 == sx, picked, own_gates)
    GP[...] = own_gates
    links.send(("gp",), GP, GPR, dev(dc=1))
    def next_piece(dx):
        links.recv(("kv", dx), K.at[0 : 2 * HB], dev(dx=-dx))
        ring_start(dx)

    for dx in pieces[1:-1]:
        next_piece(dx)
    links.recv(("gp",), GPR, dev(dc=1))
    theirs = GPR[...]
    chip_gates = jnp.zeros((8, GB), jnp.float32)
    for sx in range(X):
        a, b = own_gates[sx : sx + 1], theirs[sx : sx + 1]
        chip_gates = jnp.where(row8 == 2 * sx, jnp.where(c == 0, a, b), chip_gates)
        chip_gates = jnp.where(row8 == 2 * sx + 1, jnp.where(c == 0, b, a), chip_gates)
    G[z] = chip_gates
    for d in far_first:
        links.send(("gz",), G.at[z], G.at[z], dev(dz=d))
    for dx in pieces[-1:]:
        next_piece(dx)
    to_core(0)

    links.recv(("q",), QT.at[0 : X - 1], dev(dx=1))
    for sx in range(X):
        QB[sx, 0:HEAD_DIM, 0:GB] = QT[sx]
        QB[sx, HEAD_DIM:, GB:] = QT[sx]
    links.recv(("woz",), WO.at[:, 0 : (Z - 1) * PR, 0:WH], dev(dz=1))
    own = wo_bundle(c, x, y)
    for dx, dy in plane:
        links.send(("woxy",), own, own, dev(dx=dx, dy=dy))
    links.send(("woc",), own, own, dev(dc=1))

    def cumulative(block):
        n = block.shape[0]
        lane = lax.broadcasted_iota(jnp.int32, block.shape, 1)
        step = 1
        while step < GB:
            block = block + jnp.where(lane >= step, pltpu.roll(block, step, 1), 0.0)
            step *= 2
        total = jnp.broadcast_to(block[:, GB - 1 :], (n, LANES))
        row = lax.broadcasted_iota(jnp.int32, total.shape, 0)
        before = jnp.where(row >= 1, pltpu.roll(total, 1, 0), 0.0)
        step = 1
        while step < n:
            before = before + jnp.where(row >= step, pltpu.roll(before, step, 0), 0.0)
            step *= 2
        return (block + before[:, 0:1]) * LOG2E

    def query_sums(block):
        return [
            jnp.sum(jnp.where(row8 == 2 * sx + c, block, 0.0), axis=0, keepdims=True)
            for sx in range(X)
        ]

    def key_sums(block, cc):
        block = jnp.where(cc == 0, block, pltpu.roll(block, 7, 0))
        both = jnp.concatenate([block[:, :HB], block[:, HB:]], axis=0)
        both = jnp.concatenate([both, jnp.zeros((LANES - 16, HB), jnp.float32)], axis=0)
        return both.T

    def attend(items, cum_q):
        AHEAD, SOFT = 3, 1
        n_s, n_p = AHEAD - SOFT + 1, SOFT + 1
        best, rescale, loaded = {}, {}, {}

        def prepared(table, at, pair):
            key = (id(table), pair)
            if key not in loaded:
                even, odd = 4 * pair, 4 * pair + 2
                b0 = [table[:, even : even + 1], table[:, odd : odd + 1]]
                b1 = [table[:, 8 + even : 9 + even], table[:, 8 + odd : 9 + odd]]
                start = pl.multiple_of(at + pair * 2 * HB, 2 * HB)
                loaded[key] = jnp.concatenate(b0, axis=0), jnp.concatenate(b1, axis=0), start
            return loaded[key]

        def scores(j):
            table, at, pair, t, mask = items[j]
            b0, b1, start = prepared(table, at, pair)
            s = jnp.dot(K[pl.ds(start, 2 * HB), :], QB[t], preferred_element_type=jnp.float32)
            s0, s1 = s[:, :GB] - b0, s[:, GB:] - b1
            if mask is not None:
                s0, s1 = mask(s0, 0, t), mask(s1, 1, t)
            SC[j % n_s, 0], SC[j % n_s, 1] = s0, s1
            best[j] = jnp.maximum(jnp.max(s0, axis=0, keepdims=True), jnp.max(s1, axis=0, keepdims=True))

        def softmax(j):
            t = items[j][3]
            old = M[t]
            new = jnp.maximum(old, best[j] + cum_q[t])
            rescale[j] = jnp.exp2(old - new)
            M[t] = new
            shift = new - cum_q[t]
            PB[j % n_p, : 2 * HB] = jnp.exp2(SC[j % n_s, 0] - shift).astype(jnp.bfloat16)
            PB[j % n_p, 2 * HB :] = jnp.exp2(SC[j % n_s, 1] - shift).astype(jnp.bfloat16)

        def weigh(j):
            table, at, pair, t, _ = items[j]
            start = prepared(table, at, pair)[2]
            v = jnp.concatenate(
                [VT[0, :, pl.ds(start, 2 * HB)], VT[1, :, pl.ds(start, 2 * HB)]], axis=1
            )
            ACC[t] = ACC[t] * rescale[j] + jnp.dot(
                v, PB[j % n_p], preferred_element_type=jnp.float32
            )

        for j in range(-AHEAD, len(items)):
            if 0 <= j + AHEAD < len(items):
                scores(j + AHEAD)
            if j >= 0:
                weigh(j)
            if 0 <= j + SOFT < len(items):
                softmax(j + SOFT)

    cum_here = cumulative(G[z])
    cum_q_here = query_sums(cum_here)

    def present(cc):
        def masked(pair):
            def mask(s, which, t):
                r = lax.broadcasted_iota(jnp.int32, s.shape, 0)
                first = 4 * pair + cc
                key = jnp.where(r < HB, first * GB + r, (first + 2) * GB + r - HB) + which * HB
                query = (2 * t + c) * GB + lax.broadcasted_iota(jnp.int32, s.shape, 1)
                return jnp.where(key <= query, s, LOW)

            return mask

        table = key_sums(cum_here, cc)
        items = [
            (table, slot(cc, z, 0), pair, t, masked(pair) if t <= 2 * pair + 1 else None)
            for pair in range(X // 2)
            for t in range(2 * pair, X)
        ]
        attend(items, cum_q_here)

    def past(ds, cc):
        items = []
        for d in ds:
            zz = zrel(d)
            table = key_sums(CUM[zz], cc)
            items += [
                (table, slot(cc, zz, 0), pair, t, None) for pair in range(X // 2) for t in range(X)
            ]
        attend(items, query_sums(CUM[z]))

    def wo_rows(bundles):
        return bundles * Z * PR * WH // WO.shape[2]

    def wo_forward():
        links.recv(("woxy",), WO.at[:, 0 : wo_rows(len(plane)), :], dev(dx=1))
        for dx, dy in plane:
            theirs = wo_bundle(c, xrel(-dx), yrel(-dy))
            links.send(("woc",), theirs, theirs, dev(dc=1))

    def step_back(k, cc):
        if k == 0:
            present(cc)
        elif k < UP:

            @pl.when(z + k >= Z)
            def _():
                past([-k, k], cc)

            @pl.when((z >= k) & (z + k < Z))
            def _():
                past([-k], cc)

        else:

            @pl.when(z >= k)
            def _():
                past([-k], cc)

    def came(k):
        for d in [-k, k] if 0 < k < UP else [-k]:
            other_core(d)

    cut = (len(pieces) + 1) // 2
    for k in range(1, UP + 1):
        ring_step(k, pieces[:cut])
        step_back(k - 1, c)
        ring_step(k, pieces[cut:])
        to_core(-k)
        if k < UP:
            to_core(k)
        if k == UP:
            wo_forward()
        came(k - 1)
        step_back(k - 1, co)
        if k == 1:
            links.recv(("gz",), G.at[0 : Z - 1], dev(dz=1))
            CUM[...] = cumulative(G[...].reshape(Z * 8, GB)).reshape(Z, 8, GB)
    step_back(UP, c)
    came(UP)
    step_back(UP, co)

    for t in range(X):
        acc = ACC[t]
        o = (acc[:HEAD_DIM] / acc[HEAD_DIM : HEAD_DIM + 1]).astype(jnp.bfloat16)
        for yy in range(Y):
            part = o[:, yy * TB : (yy + 1) * TB]
            for h in range(2):
                OS[t, yy, :, h * TB : (h + 1) * TB] = part[h * HALF : (h + 1) * HALF]

    def at_rows(xx, yy):
        return AT.at[pl.ds(pl.multiple_of((yy * X + xx) * HALF, HALF), HALF), :]

    for dx, dy in plane:
        links.send(("o",), OS.at[xrel(dx), yrel(dy)], at_rows(x, y), dev(dx=dx, dy=dy))
    at_rows(x, y)[...] = OS[x, y]
    links.recv(("woc",), WO.at[:, 0 : wo_rows(X * Y), :], dev(dc=1))
    links.recv(("o",), AT.at[0 : len(plane) * HALF], dev(dx=1))

    attended = AT[...]
    for cc in range(C):
        for xx in range(X):
            block = (cc * X + xx) * Z * PR
            part = sum(
                jnp.dot(WO[h, block : block + Z * PR, :], attended, preferred_element_type=jnp.float32)[
                    :, h * TB : (h + 1) * TB
                ]
                for h in range(2)
            )
            for zz in range(Z):
                to = ((zz * X + xx) * C + cc) * PR
                PT[to : to + PR, 0:TB] = part[zz * PR : (zz + 1) * PR]
    out_ref[...] = rms_norm(PT[...].T[:TB], ogain_ref[...])
    links.drain(dev(dc=1))


def layer(dims, tokens, norm_gain, w_query, w_key, w_value, w_forget, forget_offset, w_out_t, out_gain):
    Z, X, C, Y = dims
    TB, D = tokens.shape
    PR, WC = w_query.shape
    GB = TB * Y
    HB = GB // 2
    LW = 3 * WC + LANES
    keys = Z * X * C * HB
    n_sems = 101
    vmem, smem = pl.BlockSpec(memory_space=pltpu.VMEM), pl.BlockSpec(memory_space=pltpu.SMEM)
    hbm = pl.BlockSpec(memory_space=pltpu.MemorySpace.HBM)
    bf16, f32 = jnp.bfloat16, jnp.float32
    scratch = [
        pltpu.VMEM((Z, X * C * PR, LW), bf16),
        pltpu.VMEM((GB, D), bf16),
        pltpu.VMEM((2, D, D // 2), bf16),
        pltpu.VMEM((X, HB, LANES), bf16),
        pltpu.VMEM((X, 2, HEAD_DIM, HB), bf16),
        pltpu.VMEM((X, HEAD_DIM, GB), bf16),
        pltpu.VMEM((8, GB), f32),
        pltpu.VMEM((X, 8, GB), f32),
        pltpu.VMEM((8, GB), f32),
        pltpu.VMEM((8, GB), f32),
        pltpu.VMEM((Z, 8, GB), f32),
        pltpu.VMEM((Z, 8, GB), f32),
        pltpu.VMEM((keys, LANES), bf16),
        pltpu.VMEM((2, HEAD_DIM + 16, keys), bf16),
        pltpu.VMEM((X, HEAD_DIM, GB), bf16),
        pltpu.VMEM((X, LANES, 2 * GB), bf16),
        pltpu.VMEM((X, 1, GB), f32),
        pltpu.VMEM((X, HEAD_DIM + 16, GB), f32),
        pltpu.VMEM((X, Y, HEAD_DIM // 2, 2 * TB), bf16),
        pltpu.VMEM((D // 2, 2 * TB), bf16),
        pltpu.VMEM((D, LANES), f32),
        pltpu.VMEM((3, 2, 2 * HB, GB), f32),
        pltpu.VMEM((2, 4 * HB, GB), bf16),
        pltpu.VMEM((2, PR, WC // 2), bf16),
        pltpu.VMEM((TB, D), bf16),
        pltpu.VMEM((1, D), f32),
        pltpu.VMEM((PR, WC), bf16),
        pltpu.VMEM((PR, WC), bf16),
        pltpu.VMEM((PR, WC), bf16),
        pltpu.VMEM((w_forget.shape[1], PR), bf16),
        pltpu.VMEM((PR, WC), bf16),
        pltpu.VMEM((1, D), f32),
        pltpu.SemaphoreType.DMA((8,)),
        pltpu.SemaphoreType.DMA((5,)),
        pltpu.SemaphoreType.DMA((n_sems,)),
    ]
    return pl.pallas_call(
        functools.partial(kernel, dims),
        out_shape=jax.ShapeDtypeStruct((TB, D), bf16),
        in_specs=[hbm] * 6 + [smem, hbm, hbm],
        out_specs=vmem,
        scratch_shapes=scratch,
        compiler_params=pltpu.CompilerParams(
            collective_id=0, has_side_effects=True, vmem_limit_bytes=56 * 1024 * 1024
        ),
    )(
        tokens,
        norm_gain.reshape(1, D),
        w_query,
        w_key,
        w_value,
        w_forget.T,
        forget_offset,
        w_out_t,
        out_gain.reshape(1, D),
    )


def sharded(mesh, dims):
    finer = Mesh(mesh.devices.reshape(*dims), AXES)
    sp = ("z", "x", "c")
    return jax.shard_map(
        functools.partial(layer, dims),
        mesh=finer,
        in_specs=(
            P(AXES, None),
            P(),
            P(sp, "y"),
            P(sp, "y"),
            P(sp, "y"),
            P(sp, "y"),
            P("y"),
            P(sp, "y"),
            P(),
        ),
        out_specs=P(AXES, None),
        check_vma=False,
    )


def solution(mesh):
    return sharded(mesh, (8, 4, 2, mesh.shape["tp"]))
```

```python
import functools
import math

import jax
import jax.numpy as jnp
from jax import lax
from jax.experimental import pallas as pl
from jax.experimental.pallas import tpu as pltpu
from jax.sharding import Mesh
from jax.sharding import PartitionSpec as P

HEAD_DIM = 64
AXES = ("z", "x", "c", "y")
MESH = pl.DeviceIdType.MESH
EPS = 1e-06
LOG2E = 1.4426950408889634
LOW = -1e30
LANES = 128


def rms_norm(floats, gain_row):
    scale_row = lax.rsqrt(jnp.mean(floats * floats, axis=-1, keepdims=True) + EPS)
    return (floats * scale_row * gain_row).astype(jnp.bfloat16)


def log_sigmoid(t):
    u = jnp.exp(-jnp.abs(t))
    series = u * (1.0 - u * (0.5 - u * (1.0 / 3.0 - u * 0.25)))
    return jnp.minimum(t, 0.0) - jnp.where(u < 0.01, series, jnp.log(1.0 + u))


class Links:
    def __init__(self, send_sems, recv_sems, counter):
        self.send_sems, self.recv_sems, self.counter = send_sems, recv_sems, counter
        self.ids, self.sent = {}, [0]
        self.most = counter.shape[0]

    def copy(self, key, src, dst, dev):
        return pltpu.make_async_remote_copy(
            src_ref=src,
            dst_ref=dst,
            send_sem=self.send_sems.at[len(self.sent) - 1],
            recv_sem=self.recv_sems.at[self.ids.setdefault(key, len(self.ids))],
            device_id=dev,
            device_id_type=MESH,
        )

    def send(self, key, src, dst, dev):
        rows = math.prod(src.shape) * src.dtype.itemsize // (2 * LANES)
        if self.sent[-1] + rows > self.most:
            self.sent.append(0)
        self.sent[-1] += rows
        self.copy(key, src, dst, dev).start()

    def recv(self, key, landed, dev):
        self.copy(key, landed, landed, dev).wait_recv()

    def drain(self, dev):
        for at, rows in enumerate(self.sent):
            view = self.counter.at[0:rows]
            pltpu.make_async_remote_copy(
                src_ref=view,
                dst_ref=view,
                send_sem=self.send_sems.at[at],
                recv_sem=self.recv_sems.at[0],
                device_id=dev,
                device_id_type=MESH,
            ).wait_send()


def kernel(
    dims,
    tokens_hbm,
    gain_hbm,
    wq_hbm,
    wk_hbm,
    wv_hbm,
    wf_hbm,
    off_ref,
    wo_hbm,
    ogain_hbm,
    out_ref,
    W,
    XN,
    WO,
    KS,
    VS,
    QS,
    GS,
    GX,
    GP,
    GPR,
    G,
    CUM,
    K,
    VT,
    QT,
    QB,
    M,
    ACC,
    OS,
    AT,
    PT,
    SC,
    PB,
    WO_OWN,
    tokens_ref,
    gain_ref,
    wq_ref,
    wk_ref,
    wv_ref,
    wf_ref,
    wo_ref,
    ogain_ref,
    in_sems,
    send_sems,
    recv_sems,
):
    Z, X, C, Y = dims
    TB, D = tokens_hbm.shape
    GB = TB * Y
    HB = GB // 2
    PR, WC = wo_hbm.shape
    LW = W.shape[2]
    z, x, c, y = (lax.axis_index(a) for a in AXES)
    links = Links(send_sems, recv_sems, K)

    def dev(dz=0, dx=0, dc=0, dy=0):
        return {
            "z": lax.rem(z + (dz % Z), Z),
            "x": lax.rem(x + (dx % X), X),
            "c": lax.rem(c + (dc % C), C),
            "y": lax.rem(y + (dy % Y), Y),
        }

    def zrel(d):
        return lax.rem(z + (d % Z), Z)

    def xrel(d):
        return lax.rem(x + (d % X), X)

    def yrel(d):
        return lax.rem(y + (d % Y), Y)

    co = 1 - c
    plane = [(dx, dy) for dx in range(X) for dy in range(Y) if (dx, dy) != (0, 0)]
    plane.sort(key=lambda at: -min(at[0], X - at[0]) - min(at[1], Y - at[1]))
    x_far = sorted(range(1, X), key=lambda d: -min(d, X - d))
    far_first = sorted(range(1, Z), key=lambda d: -min(d, Z - d))
    near_first = [0] + far_first[::-1]
    x_near, y_near = ([1] if n == 2 else [1, -1] for n in (X, Y))

    barrier = pltpu.get_barrier_semaphore()
    greeted = (
        [dict(dx=dx, dy=dy) for dx, dy in plane] + [dict(dc=1)] + [dict(dz=d) for d in range(1, Z)]
    )
    for g in greeted:
        pl.semaphore_signal(barrier, inc=1, device_id=dev(**g), device_id_type=MESH)

    operands = (
        (wk_hbm, wk_ref),
        (wv_hbm, wv_ref),
        (wq_hbm, wq_ref),
        (wf_hbm, wf_ref),
        (tokens_hbm, tokens_ref),
        (gain_hbm, gain_ref),
        (wo_hbm, wo_ref),
        (ogain_hbm, ogain_ref),
    )
    fetches = [
        pltpu.make_async_copy(src, dst, in_sems.at[i]) for i, (src, dst) in enumerate(operands)
    ]
    for fetch in fetches:
        fetch.start()
    for fetch in fetches:
        fetch.wait()

    def w_rows(xx, cc):
        return pl.ds(pl.multiple_of((xx * C + cc) * PR, PR), PR)

    KVF, Q = (0, 2 * WC + LANES), (2 * WC + LANES, LW)
    mine = w_rows(x, c)
    W[z, mine, 0:WC] = wk_ref[...]
    W[z, mine, WC : 2 * WC] = wv_ref[...]
    W[z, mine, KVF[1] :] = wq_ref[...]
    PT[0:LANES] = jnp.zeros((LANES, LANES), jnp.float32)
    PT[0:X, 0:PR] = wf_ref[...].astype(jnp.float32)
    W[z, mine, 2 * WC : KVF[1]] = PT[0:LANES].T[:PR].astype(jnp.bfloat16)

    def t_rows(yy, lo=0, count=TB):
        return XN.at[pl.ds(pl.multiple_of(yy * TB + lo, 32), count), :]

    t_rows(y)[...] = rms_norm(tokens_ref[...].astype(jnp.float32), gain_ref[...])

    HALF = HEAD_DIM // 2
    WH = WC // 2

    def wo_columns(yy):
        return pl.ds(pl.multiple_of(yy * WH, WH), WH)

    def wo_block(cc, xx, zz, yy):
        row = ((cc * X + xx) * Z + zz) * PR
        return WO.at[:, pl.ds(pl.multiple_of(row, PR), PR), wo_columns(yy)]

    def wo_bundle(cc, xx, yy):
        row = (cc * X + xx) * Z * PR
        return WO.at[:, pl.ds(pl.multiple_of(row, PR), Z * PR), wo_columns(yy)]

    own_wo = wo_ref[...].astype(jnp.float32)
    for h in range(2):
        cols = [own_wo[:, i * HALF : (i + 1) * HALF] for i in range(h, 2 * X, 2)]
        WO_OWN[h] = jnp.concatenate(cols, axis=1).astype(jnp.bfloat16)
    wo_block(c, x, z, y)[...] = WO_OWN[...]
    pl.semaphore_wait(barrier, len(greeted))

    def w_unit(d, xx, cc, lanes):
        return W.at[zrel(d), w_rows(xx, cc), lanes[0] : lanes[1]]

    def w_bundle(xx, cc, lanes):
        return W.at[:, w_rows(xx, cc), lanes[0] : lanes[1]]

    def halves(lanes):
        middle = lanes[0] + -(-(lanes[1] - lanes[0]) // (2 * LANES)) * LANES
        return (lanes[0], middle), (middle, lanes[1])

    opposite = X > 2

    def fine_z(d):
        if d != 0:
            links.recv(("wz", d), w_unit(-d, x, c, KVF), dev(dz=-d))
        for dx in x_near:
            unit = w_unit(-d, x, c, KVF)
            links.send(("x1", d, dx), unit, unit, dev(dx=dx))

    def fine_x(d):
        for dx, part in zip(x_near, halves(KVF)):
            links.recv(("x1", d, dx), w_unit(-d, xrel(-dx), c, KVF), dev(dx=-dx))
            if opposite:
                unit = w_unit(-d, xrel(-dx), c, part)
                links.send(("x2", d, dx), unit, unit, dev(dx=dx))

    def fine_last(d):
        for dx, part in zip(x_near, halves(KVF)):
            links.recv(("x2", d, dx), w_unit(-d, xrel(2), c, part), dev(dx=-dx))
        unit = w_unit(-d, xrel(2), c, KVF)
        links.send(("wc", KVF), unit, unit, dev(dc=1))

    def to_other_core(xx, lanes):
        view = w_bundle(xx, c, lanes)
        links.send(("wc", lanes), view, view, dev(dc=1))

    def core_last(lanes):
        links.recv(("wc", lanes), W.at[:, 0 : X * PR, lanes[0] : lanes[1]], dev(dc=1))

    for lanes in (KVF, Q):
        for d in far_first:
            unit = w_unit(0, x, c, lanes)
            links.send(("wz", d if lanes == KVF else Q), unit, unit, dev(dz=d))
    for dy in y_near:
        links.send(("tok", dy), t_rows(y), t_rows(y), dev(dy=dy))
    for d in far_first:
        links.send(("woz",), WO_OWN, wo_block(c, x, z, y), dev(dz=d))

    QB[...] = jnp.zeros_like(QB)
    VT[:, HEAD_DIM:, :] = jnp.ones((2, VT.shape[1] - HEAD_DIM, VT.shape[2]), jnp.bfloat16)
    M[...] = jnp.full(M.shape, LOW, jnp.float32)
    ACC[...] = jnp.zeros_like(ACC)

    for d in near_first:
        fine_z(d)
    to_other_core(x, KVF)
    for dy, lo in zip(y_near, (0, TB // 2)):
        links.recv(("tok", dy), t_rows(yrel(-dy)), dev(dy=-dy))
        if Y > 2:
            part = t_rows(yrel(-dy), lo, TB // 2)
            links.send(("tok2", dy), part, part, dev(dy=dy))
    links.recv(("wz", Q), W.at[0 : Z - 1, 0:PR, Q[0] : Q[1]], dev(dz=1))
    for dx in x_near:
        view = w_bundle(x, c, Q)
        links.send(("x1", Q, dx), view, view, dev(dx=dx))
    for d in near_first:
        fine_x(d)
    for dx in x_near:
        to_other_core(xrel(-dx), KVF)
    if opposite:
        for d in near_first:
            fine_last(d)
    for dx, part in zip(x_near, halves(Q)):
        links.recv(("x1", Q, dx), w_bundle(xrel(-dx), c, Q), dev(dx=-dx))
        if opposite:
            view = w_bundle(xrel(-dx), c, part)
            links.send(("x2", Q, dx), view, view, dev(dx=dx))
    for dx in [0] + x_near:
        to_other_core(xrel(-dx), Q)
    if Y > 2:
        for dy, lo in zip(y_near, (0, TB // 2)):
            links.recv(("tok2", dy), t_rows(yrel(2), lo, TB // 2), dev(dy=-dy))
    core_last(KVF)

    rows = XN[...]

    def project(lo, count):
        weight = W[:, :, lo : lo + count].reshape(D, count)
        return jnp.dot(rows, weight, preferred_element_type=jnp.float32)

    def slot(cc, zz, xx):
        return ((cc * Z + zz) * X + xx) * HB

    def k_block(cc, zz, xx):
        return K.at[pl.ds(pl.multiple_of(slot(cc, zz, xx), LANES), HB), :]

    def v_block(cc, zz, xx):
        return VT.at[:, 0:HEAD_DIM, pl.ds(pl.multiple_of(slot(cc, zz, xx), LANES), HB)]

    gates = project(2 * WC, LANES).T[:8]
    head_row = lax.broadcasted_iota(jnp.int32, gates.shape, 0)
    offset = jnp.zeros_like(gates)
    for h in range(X):
        offset = jnp.where(head_row == h, off_ref[h], offset)
    GS[...] = log_sigmoid(gates + offset + math.log(GB * Z * X * C))
    for dx in x_far:
        links.send(("g",), GS, GX.at[x], dev(dx=dx))
    GX[x] = GS[...]
    k_all = project(0, WC)
    for h in range(X):
        kh = k_all[:, h * HEAD_DIM : (h + 1) * HEAD_DIM]
        KS[h] = jnp.concatenate([kh[:HB], kh[HB:]], axis=1).astype(jnp.bfloat16)
    for dx in range(1, X):
        links.send(("kv", dx), KS.at[xrel(dx)], k_block(c, z, x), dev(dx=dx))
    if opposite:
        for dx, part in zip(x_near, halves(Q)):
            links.recv(("x2", Q, dx), w_bundle(xrel(2), c, part), dev(dx=-dx))
        to_other_core(xrel(2), Q)
    v_all = project(WC, WC).T
    for h in range(X):
        vh = v_all[h * HEAD_DIM : (h + 1) * HEAD_DIM].astype(jnp.bfloat16)
        VS[h, 0] = vh[:, :HB]
        VS[h, 1] = vh[:, HB:]
    for dx in range(1, X):
        links.send(("kv", dx), VS.at[xrel(dx)], v_block(c, z, x), dev(dx=dx))
    k_block(c, z, x)[...] = KS[x]
    v_block(c, z, x)[...] = VS[x]

    UP = DN = Z // 2

    def goes(way, a, k):
        return k < UP or (k == UP and (a == 0) == (way == "up"))

    def bundle(zz, cc):
        at = pl.multiple_of(slot(cc, zz, 0), LANES)
        return K.at[pl.ds(at, X * HB), :], VT.at[:, 0:HEAD_DIM, pl.ds(at, X * HB)]

    def piece(zz, dx):
        return k_block(c, zz, xrel(-dx)), v_block(c, zz, xrel(-dx))

    WAYS = (("up", 1), ("dn", -1))
    pieces = [0] + ([1, X - 1] if X > 2 else [1]) + list(range(2, X - 1))

    def ring_start(dx):
        for a, view in enumerate(piece(z, dx)):
            for way, sign in WAYS:
                if goes(way, a, 1):
                    links.send((way, 1, dx), view, view, dev(dz=sign))

    def to_core(d):
        for view in bundle(zrel(d), c):
            links.send(("core", d % Z), view, view, dev(dc=1))

    def ring_step(k, some):
        for dx in some:
            for way, sign in WAYS:
                arrays = [a for a in range(2) if goes(way, a, k)]
                links.recv((way, k, dx), K.at[0 : len(arrays) * HB], dev(dz=-sign))
                for a in arrays:
                    if goes(way, a, k + 1):
                        view = piece(zrel(-sign * k), dx)[a]
                        links.send((way, k + 1, dx), view, view, dev(dz=sign))

    def other_core(d):
        links.recv(("core", d % Z), K.at[0 : 2 * X * HB], dev(dc=1))

    ring_start(0)
    core_last(Q)
    q_all = project(KVF[1], WC)
    q_all = q_all.astype(jnp.bfloat16).astype(jnp.float32) * (HEAD_DIM**-0.5 * LOG2E)
    q_all = q_all.T
    for h in range(X):
        QS[h] = q_all[h * HEAD_DIM : (h + 1) * HEAD_DIM].astype(jnp.bfloat16)
    for dx in x_far:
        links.send(("q",), QS.at[xrel(dx)], QT.at[x], dev(dx=dx))
    QT[x] = QS[x]

    links.recv(("g",), GX.at[0 : X - 1], dev(dx=1))
    row8 = lax.broadcasted_iota(jnp.int32, (8, GB), 0)
    own_gates = jnp.zeros((8, GB), jnp.float32)
    for sx in range(X):
        picked = jnp.sum(jnp.where(row8 == x, GX[sx], 0.0), axis=0, keepdims=True)
        own_gates = jnp.where(row8 == sx, picked, own_gates)
    GP[...] = own_gates
    links.send(("gp",), GP, GPR, dev(dc=1))
    def next_piece(dx):
        links.recv(("kv", dx), K.at[0 : 2 * HB], dev(dx=-dx))
        ring_start(dx)

    for dx in pieces[1:-1]:
        next_piece(dx)
    links.recv(("gp",), GPR, dev(dc=1))
    theirs = GPR[...]
    chip_gates = jnp.zeros((8, GB), jnp.float32)
    for sx in range(X):
        a, b = own_gates[sx : sx + 1], theirs[sx : sx + 1]
        chip_gates = jnp.where(row8 == 2 * sx, jnp.where(c == 0, a, b), chip_gates)
        chip_gates = jnp.where(row8 == 2 * sx + 1, jnp.where(c == 0, b, a), chip_gates)
    G[z] = chip_gates
    for d in far_first:
        links.send(("gz",), G.at[z], G.at[z], dev(dz=d))
    for dx in pieces[-1:]:
        next_piece(dx)
    to_core(0)

    links.recv(("q",), QT.at[0 : X - 1], dev(dx=1))
    for sx in range(X):
        QB[sx, 0:HEAD_DIM, 0:GB] = QT[sx]
        QB[sx, HEAD_DIM:, GB:] = QT[sx]
    links.recv(("woz",), WO.at[:, 0 : (Z - 1) * PR, 0:WH], dev(dz=1))
    own = wo_bundle(c, x, y)
    for dx, dy in plane:
        links.send(("woxy",), own, own, dev(dx=dx, dy=dy))
    links.send(("woc",), own, own, dev(dc=1))

    def cumulative(block):
        n = block.shape[0]
        lane = lax.broadcasted_iota(jnp.int32, block.shape, 1)
        step = 1
        while step < GB:
            block = block + jnp.where(lane >= step, pltpu.roll(block, step, 1), 0.0)
            step *= 2
        total = jnp.broadcast_to(block[:, GB - 1 :], (n, LANES))
        row = lax.broadcasted_iota(jnp.int32, total.shape, 0)
        before = jnp.where(row >= 1, pltpu.roll(total, 1, 0), 0.0)
        step = 1
        while step < n:
            before = before + jnp.where(row >= step, pltpu.roll(before, step, 0), 0.0)
            step *= 2
        return (block + before[:, 0:1]) * LOG2E

    def query_sums(block):
        return [
            jnp.sum(jnp.where(row8 == 2 * sx + c, block, 0.0), axis=0, keepdims=True)
            for sx in range(X)
        ]

    def key_sums(block, cc):
        block = jnp.where(cc == 0, block, pltpu.roll(block, 7, 0))
        both = jnp.concatenate([block[:, :HB], block[:, HB:]], axis=0)
        both = jnp.concatenate([both, jnp.zeros((LANES - 16, HB), jnp.float32)], axis=0)
        return both.T

    def attend(items, cum_q):
        AHEAD, SOFT = 3, 1
        n_s, n_p = AHEAD - SOFT + 1, SOFT + 1
        best, rescale, loaded = {}, {}, {}

        def prepared(table, at, pair):
            key = (id(table), pair)
            if key not in loaded:
                even, odd = 4 * pair, 4 * pair + 2
                b0 = [table[:, even : even + 1], table[:, odd : odd + 1]]
                b1 = [table[:, 8 + even : 9 + even], table[:, 8 + odd : 9 + odd]]
                start = pl.multiple_of(at + pair * 2 * HB, 2 * HB)
                loaded[key] = jnp.concatenate(b0, axis=0), jnp.concatenate(b1, axis=0), start
            return loaded[key]

        def scores(j):
            table, at, pair, t, mask = items[j]
            b0, b1, start = prepared(table, at, pair)
            s = jnp.dot(K[pl.ds(start, 2 * HB), :], QB[t], preferred_element_type=jnp.float32)
            s0, s1 = s[:, :GB] - b0, s[:, GB:] - b1
            if mask is not None:
                s0, s1 = mask(s0, 0, t), mask(s1, 1, t)
            SC[j % n_s, 0], SC[j % n_s, 1] = s0, s1
            best[j] = jnp.maximum(jnp.max(s0, axis=0, keepdims=True), jnp.max(s1, axis=0, keepdims=True))

        def softmax(j):
            t = items[j][3]
            old = M[t]
            new = jnp.maximum(old, best[j] + cum_q[t])
            rescale[j] = jnp.exp2(old - new)
            M[t] = new
            shift = new - cum_q[t]
            PB[j % n_p, : 2 * HB] = jnp.exp2(SC[j % n_s, 0] - shift).astype(jnp.bfloat16)
            PB[j % n_p, 2 * HB :] = jnp.exp2(SC[j % n_s, 1] - shift).astype(jnp.bfloat16)

        def weigh(j):
            table, at, pair, t, _ = items[j]
            start = prepared(table, at, pair)[2]
            v = jnp.concatenate(
                [VT[0, :, pl.ds(start, 2 * HB)], VT[1, :, pl.ds(start, 2 * HB)]], axis=1
            )
            ACC[t] = ACC[t] * rescale[j] + jnp.dot(
                v, PB[j % n_p], preferred_element_type=jnp.float32
            )

        for j in range(-AHEAD, len(items)):
            if 0 <= j + AHEAD < len(items):
                scores(j + AHEAD)
            if j >= 0:
                weigh(j)
            if 0 <= j + SOFT < len(items):
                softmax(j + SOFT)

    cum_here = cumulative(G[z])
    cum_q_here = query_sums(cum_here)

    def present(cc):
        def masked(pair):
            def mask(s, which, t):
                r = lax.broadcasted_iota(jnp.int32, s.shape, 0)
                first = 4 * pair + cc
                key = jnp.where(r < HB, first * GB + r, (first + 2) * GB + r - HB) + which * HB
                query = (2 * t + c) * GB + lax.broadcasted_iota(jnp.int32, s.shape, 1)
                return jnp.where(key <= query, s, LOW)

            return mask

        table = key_sums(cum_here, cc)
        items = [
            (table, slot(cc, z, 0), pair, t, masked(pair) if t <= 2 * pair + 1 else None)
            for pair in range(X // 2)
            for t in range(2 * pair, X)
        ]
        attend(items, cum_q_here)

    def past(ds, cc):
        items = []
        for d in ds:
            zz = zrel(d)
            table = key_sums(CUM[zz], cc)
            items += [
                (table, slot(cc, zz, 0), pair, t, None) for pair in range(X // 2) for t in range(X)
            ]
        attend(items, query_sums(CUM[z]))

    def wo_rows(bundles):
        return bundles * Z * PR * WH // WO.shape[2]

    def wo_forward():
        links.recv(("woxy",), WO.at[:, 0 : wo_rows(len(plane)), :], dev(dx=1))
        for dx, dy in plane:
            theirs = wo_bundle(c, xrel(-dx), yrel(-dy))
            links.send(("woc",), theirs, theirs, dev(dc=1))

    def step_back(k, cc):
        if k == 0:
            present(cc)
        elif k < UP:

            @pl.when(z + k >= Z)
            def _():
                past([-k, k], cc)

            @pl.when((z >= k) & (z + k < Z))
            def _():
                past([-k], cc)

        else:

            @pl.when(z >= k)
            def _():
                past([-k], cc)

    def came(k):
        for d in [-k, k] if 0 < k < UP else [-k]:
            other_core(d)

    cut = (len(pieces) + 1) // 2
    for k in range(1, UP + 1):
        ring_step(k, pieces[:cut])
        step_back(k - 1, c)
        ring_step(k, pieces[cut:])
        to_core(-k)
        if k < UP:
            to_core(k)
        if k == UP:
            wo_forward()
        came(k - 1)
        step_back(k - 1, co)
        if k == 1:
            links.recv(("gz",), G.at[0 : Z - 1], dev(dz=1))
            CUM[...] = cumulative(G[...].reshape(Z * 8, GB)).reshape(Z, 8, GB)
    step_back(UP, c)
    came(UP)
    step_back(UP, co)

    for t in range(X):
        acc = ACC[t]
        o = (acc[:HEAD_DIM] / acc[HEAD_DIM : HEAD_DIM + 1]).astype(jnp.bfloat16)
        for yy in range(Y):
            part = o[:, yy * TB : (yy + 1) * TB]
            for h in range(2):
                OS[t, yy, :, h * TB : (h + 1) * TB] = part[h * HALF : (h + 1) * HALF]

    def at_rows(xx, yy):
        return AT.at[pl.ds(pl.multiple_of((yy * X + xx) * HALF, HALF), HALF), :]

    for dx, dy in plane:
        links.send(("o",), OS.at[xrel(dx), yrel(dy)], at_rows(x, y), dev(dx=dx, dy=dy))
    at_rows(x, y)[...] = OS[x, y]
    links.recv(("woc",), WO.at[:, 0 : wo_rows(X * Y), :], dev(dc=1))
    links.recv(("o",), AT.at[0 : len(plane) * HALF], dev(dx=1))

    attended = AT[...]
    for cc in range(C):
        for xx in range(X):
            block = (cc * X + xx) * Z * PR
            part = sum(
                jnp.dot(WO[h, block : block + Z * PR, :], attended, preferred_element_type=jnp.float32)[
                    :, h * TB : (h + 1) * TB
                ]
                for h in range(2)
            )
            for zz in range(Z):
                to = ((zz * X + xx) * C + cc) * PR
                PT[to : to + PR, 0:TB] = part[zz * PR : (zz + 1) * PR]
    out_ref[...] = rms_norm(PT[...].T[:TB], ogain_ref[...])
    links.drain(dev(dc=1))


def layer(dims, tokens, norm_gain, w_query, w_key, w_value, w_forget, forget_offset, w_out_t, out_gain):
    Z, X, C, Y = dims
    TB, D = tokens.shape
    PR, WC = w_query.shape
    GB = TB * Y
    HB = GB // 2
    LW = 3 * WC + LANES
    keys = Z * X * C * HB
    n_sems = 101
    vmem, smem = pl.BlockSpec(memory_space=pltpu.VMEM), pl.BlockSpec(memory_space=pltpu.SMEM)
    hbm = pl.BlockSpec(memory_space=pltpu.MemorySpace.HBM)
    bf16, f32 = jnp.bfloat16, jnp.float32
    scratch = [
        pltpu.VMEM((Z, X * C * PR, LW), bf16),
        pltpu.VMEM((GB, D), bf16),
        pltpu.VMEM((2, D, D // 2), bf16),
        pltpu.VMEM((X, HB, LANES), bf16),
        pltpu.VMEM((X, 2, HEAD_DIM, HB), bf16),
        pltpu.VMEM((X, HEAD_DIM, GB), bf16),
        pltpu.VMEM((8, GB), f32),
        pltpu.VMEM((X, 8, GB), f32),
        pltpu.VMEM((8, GB), f32),
        pltpu.VMEM((8, GB), f32),
        pltpu.VMEM((Z, 8, GB), f32),
        pltpu.VMEM((Z, 8, GB), f32),
        pltpu.VMEM((keys, LANES), bf16),
        pltpu.VMEM((2, HEAD_DIM + 16, keys), bf16),
        pltpu.VMEM((X, HEAD_DIM, GB), bf16),
        pltpu.VMEM((X, LANES, 2 * GB), bf16),
        pltpu.VMEM((X, 1, GB), f32),
        pltpu.VMEM((X, HEAD_DIM + 16, GB), f32),
        pltpu.VMEM((X, Y, HEAD_DIM // 2, 2 * TB), bf16),
        pltpu.VMEM((D // 2, 2 * TB), bf16),
        pltpu.VMEM((D, LANES), f32),
        pltpu.VMEM((3, 2, 2 * HB, GB), f32),
        pltpu.VMEM((2, 4 * HB, GB), bf16),
        pltpu.VMEM((2, PR, WC // 2), bf16),
        pltpu.VMEM((TB, D), bf16),
        pltpu.VMEM((1, D), f32),
        pltpu.VMEM((PR, WC), bf16),
        pltpu.VMEM((PR, WC), bf16),
        pltpu.VMEM((PR, WC), bf16),
        pltpu.VMEM((w_forget.shape[1], PR), bf16),
        pltpu.VMEM((PR, WC), bf16),
        pltpu.VMEM((1, D), f32),
        pltpu.SemaphoreType.DMA((8,)),
        pltpu.SemaphoreType.DMA((5,)),
        pltpu.SemaphoreType.DMA((n_sems,)),
    ]
    return pl.pallas_call(
        functools.partial(kernel, dims),
        out_shape=jax.ShapeDtypeStruct((TB, D), bf16),
        in_specs=[hbm] * 6 + [smem, hbm, hbm],
        out_specs=vmem,
        scratch_shapes=scratch,
        compiler_params=pltpu.CompilerParams(
            collective_id=0, has_side_effects=True, vmem_limit_bytes=56 * 1024 * 1024
        ),
    )(
        tokens,
        norm_gain.reshape(1, D),
        w_query,
        w_key,
        w_value,
        w_forget.T,
        forget_offset,
        w_out_t,
        out_gain.reshape(1, D),
    )


def sharded(mesh, dims):
    finer = Mesh(mesh.devices.reshape(*dims), AXES)
    sp = ("z", "x", "c")
    return jax.shard_map(
        functools.partial(layer, dims),
        mesh=finer,
        in_specs=(
            P(AXES, None),
            P(),
            P(sp, "y"),
            P(sp, "y"),
            P(sp, "y"),
            P(sp, "y"),
            P("y"),
            P(sp, "y"),
            P(),
        ),
        out_specs=P(AXES, None),
        check_vma=False,
    )


def solution(mesh):
    return sharded(mesh, (8, 4, 2, mesh.shape["tp"]))
```
